32 devices in a mesh: dp: 4 (over y, x), kv: 4 (over z), tp: 2 (over core).
Axes of the slice: x: 2, y: 2, z: 4, core: 2. Of those that a mesh axis runs over, the one named last changes fastest.
Arguments:
- tokens: bfloat16 [64, 2048], P('dp', ('kv', 'tp')), may hold values from -30 to 30
- state: float32 [64, 4, 256, 512], P(('dp', 'kv'), 'tp'), may hold values from -6 to 6
- mix_gain: float32 [2048], P('kv'), may hold values from 0.1 to 1.9
- w_query: bfloat16 [2048, 1024], P('kv', 'tp'), may hold values from -0.125 to 0.125
- w_key: bfloat16 [2048, 1024], P('kv', 'tp'), may hold values from -0.125 to 0.125
- w_decay: bfloat16 [2048, 1024], P('kv', 'tp'), may hold values from -0.125 to 0.125
- w_value: bfloat16 [2048, 2048], P('kv', 'tp'), may hold values from -0.125 to 0.125
- w_gate: bfloat16 [2048, 2048], P('kv', 'tp'), may hold values from -0.125 to 0.125
- decay_offset: float32 [1024], P('tp'), may hold values from -1 to 4
- head_gain: float32 [512], replicated, may hold values from 0.1 to 1.9
- w_out: bfloat16 [2048, 2048], P('tp', 'kv'), may hold values from -0.125 to 0.125
- mlp_gain: float32 [2048], replicated, may hold values from 0.1 to 1.9
- w_up: bfloat16 [2048, 8192], P(None, ('kv', 'tp')), may hold values from -0.125 to 0.125
- w_down: bfloat16 [8192, 2048], P(('kv', 'tp')), may hold values from -0.09375 to 0.09375
Outputs:
- mixed: bfloat16 [64, 2048], P('dp', ('kv', 'tp'))
- new_state: float32 [64, 4, 256, 512], P(('dp', 'kv'), 'tp')
The draws below stay inside these ranges and needn't reach their ends.
All inputs are finite; a program needn't handle non-finite values.
Results may differ from the reference program's by a relative error of at most 0.013.
Values may be sent and summed in bfloat16 or wider, within the bound.
No kernel may reach another device: no remote copies, remote signals or barrier semaphores. Data moves between devices by JAX's collectives and lax.ppermute only.
A program may use at most 64 MiB of HBM per device.

```python
import math
import jax
import jax.numpy as jnp
from jax import lax

D = 2048
HEADS = 4
KEY_DIM = 256
VAL_DIM = 512
FF = 8192
BATCH = 64


def draw_tokens(key, part):
    base_key, row_key = jax.random.split(key)
    columns = jnp.exp(jnp.linspace(math.log(0.4), math.log(2.4), D)).astype(jnp.float32)
    base = jnp.clip(jax.random.normal(base_key, (BATCH, D), jnp.float32), -6.0, 6.0)
    rowwise = jnp.exp(jax.random.uniform(row_key, (BATCH,), jnp.float32, math.log(0.5), math.log(2.0)))
    return (base * rowwise[:, None] * columns[None, :]).astype(jnp.bfloat16)


def strengthened(entries, key, source, target, blocks, factor):
    owner, partner = [(jnp.arange(entries.shape[dim]) // (entries.shape[dim] // blocks)).reshape([-1 if axis == dim else 1 for axis in range(entries.ndim)]) for dim in (source, target)]
    chosen = jax.random.permutation(key, blocks)[partner]
    strong = (owner == chosen) | (owner == (partner + blocks // 2) % blocks)
    return jnp.where(strong, factor * entries, entries)


def shard_levels(key, shape, shards, smallest, largest):
    factor_of = 1.0
    for axis_at, parts in shards:
        heights = jax.random.uniform(jax.random.fold_in(jax.random.fold_in(key, 6), axis_at), (parts,), jnp.float32, smallest / len(shards), largest / len(shards))
        factor_of = factor_of * jnp.repeat(jnp.exp(heights), shape[axis_at] // parts).reshape((-1,) + (1,) * (len(shape) - 1 - axis_at))
    return factor_of


def centred(stream_key, dims, scale, most, shards=(), kind=jnp.bfloat16):
    array = jax.random.normal(stream_key, dims, jnp.float32) * scale
    if len(shards) > 0:
        array = shard_levels(stream_key, dims, shards, -0.22, 0.18) * array
    return jnp.clip(array, min=-most, max=most).astype(kind)


def heavy_noise(rng, extent, scale, limit, cuts, heavy, held_as=jnp.bfloat16):
    entries = scale * jax.random.normal(rng, extent, jnp.float32)
    if cuts:
        entries = entries * shard_levels(rng, extent, cuts, -0.22, 0.18)
    return jnp.clip(strengthened(entries, jax.random.fold_in(rng, 3), *heavy), -limit, limit).astype(held_as)


def setup_inputs(seed: int = 0) -> dict:
    key_list = jax.random.split(jax.random.key(seed), 15)
    return {
        "tokens": draw_tokens(jax.random.fold_in(key_list[14], 71), 0),
        "state": centred(key_list[1], (BATCH, HEADS, KEY_DIM, VAL_DIM), 1.0, 6.0, ((0, 16), (1, 2)), jnp.float32),
        "mix_gain": jnp.clip(1.0 + 0.18 * jax.random.normal(key_list[2], (D,), jnp.float32), 0.1, 1.9),
        "w_query": centred(key_list[3], (D, HEADS * KEY_DIM), D ** -0.5, 0.125, ((0, 4), (1, 2))),
        "w_key": centred(key_list[4], (D, HEADS * KEY_DIM), D ** -0.5, 0.125, ((0, 4), (1, 2))),
        "w_decay": centred(key_list[5], (D, HEADS * KEY_DIM), D ** -0.5, 0.125, ((0, 4), (1, 2))),
        "w_value": centred(key_list[6], (D, HEADS * VAL_DIM), D ** -0.5, 0.125, ((0, 4), (1, 2))),
        "w_gate": centred(key_list[7], (D, HEADS * VAL_DIM), D ** -0.5, 0.125, ((0, 4), (1, 2))),
        "decay_offset": jnp.clip(-1.0 + 5.0 * jax.random.uniform(key_list[8], (HEADS * KEY_DIM,), jnp.float32) ** shard_levels(key_list[8], (HEADS * KEY_DIM,), ((0, 2),), -0.2, 0.2), -1.0, 4.0),
        "head_gain": jnp.clip(1.0 + 0.18 * jax.random.normal(key_list[9], (VAL_DIM,), jnp.float32), 0.1, 1.9),
        "w_out": centred(key_list[10], (HEADS * VAL_DIM, D), (HEADS * VAL_DIM) ** -0.5, 0.125, ((0, 2), (1, 4))),
        "mlp_gain": jnp.clip(1.0 + 0.18 * jax.random.normal(key_list[11], (D,), jnp.float32), 0.1, 1.9),
        "w_up": centred(key_list[12], (D, FF), D ** -0.5, 0.125, ((1, 8),)),
        "w_down": heavy_noise(key_list[13], (FF, D), FF ** -0.5, 0.09375, ((0, 8),), (0, 1, 8, 2.0)),
    }


epsilon = 1e-06

def reference(tokens, state, mix_gain, w_query, w_key, w_decay, w_value, w_gate, decay_offset, head_gain, w_out, mlp_gain, w_up, w_down):
    tok_float = tokens.astype(jnp.float32)
    row_scale = lax.rsqrt(lax.optimization_barrier(jnp.mean(tok_float * tok_float, axis=1, keepdims=True)) + epsilon)
    scaled = (tok_float * mix_gain).astype(jnp.bfloat16)

    def project(weight):
        return jnp.dot(scaled, weight, preferred_element_type=jnp.float32) * row_scale
    queries = (project(w_query) * KEY_DIM ** (-0.5)).reshape(BATCH, HEADS, KEY_DIM)
    new_keys = project(w_key).reshape(BATCH, HEADS, KEY_DIM)
    values = project(w_value).reshape(BATCH, HEADS, VAL_DIM)
    gates = project(w_gate)
    retain = jax.nn.sigmoid(project(w_decay) + decay_offset).reshape(BATCH, HEADS, KEY_DIM)
    new_state = retain[..., None] * state + new_keys[..., None] * values[:, :, None, :]
    readout = jnp.einsum('bhk,bhkv->bhv', queries, new_state, precision=lax.Precision.HIGHEST)
    readout = readout * lax.rsqrt(lax.optimization_barrier(jnp.mean(readout * readout, axis=2, keepdims=True)) + epsilon) * head_gain
    gated = (readout.reshape(BATCH, HEADS * VAL_DIM) * jax.nn.silu(gates)).astype(jnp.bfloat16)
    stream = (tok_float + jnp.dot(gated, w_out, preferred_element_type=jnp.float32)).astype(jnp.bfloat16)
    stream_float = stream.astype(jnp.float32)
    mlp_scale = lax.rsqrt(lax.optimization_barrier(jnp.mean(stream_float * stream_float, axis=1, keepdims=True)) + epsilon)
    normed = (stream_float * mlp_gain).astype(jnp.bfloat16)
    hidden = jnp.dot(normed, w_up, preferred_element_type=jnp.float32) * mlp_scale
    squared = jnp.square(jax.nn.relu(hidden)).astype(jnp.bfloat16)
    mixed = (stream_float + jnp.dot(squared, w_down, preferred_element_type=jnp.float32)).astype(jnp.bfloat16)
    return (mixed, new_state)
```

```python
import jax
import jax.numpy as jnp
from jax import lax
from jax.sharding import PartitionSpec as P

epsilon = 1e-06


def swap_cores(value):
    return lax.ppermute(value, "tp", [(0, 1), (1, 0)])


def spread(pieces, kv_size, me):
    if kv_size <= 8:
        return [pieces[0]] + [
            lax.ppermute(pieces[k], "kv", [(i, i ^ k) for i in range(kv_size)])
            for k in range(1, kv_size)
        ]
    order = jnp.arange(kv_size) ^ me
    sent = jnp.take(jnp.stack(pieces), order, axis=0)
    came = jnp.take(lax.all_to_all(sent, "kv", 0, 0, tiled=True), order, axis=0)
    return [came[k] for k in range(kv_size)]


def shards(kv_size, tokens, state, mix_gain, w_query, w_key, w_decay, w_value, w_gate, decay_offset, head_gain,
           w_out, mlp_gain, w_up, w_down):
    seq_dev, heads_here, key_dim, val_dim = state.shape
    own_width = tokens.shape[1]
    me = lax.axis_index("kv")
    core = lax.axis_index("tp")
    depth = 2 * own_width * kv_size
    bf16, f32 = jnp.bfloat16, jnp.float32

    other = swap_cores(tokens)
    tok_cols = jnp.where(core == 0, jnp.concatenate([tokens, other], 1), jnp.concatenate([other, tokens], 1))
    tok_float = tok_cols.astype(f32)
    squares = jnp.sum(tok_float * tok_float, axis=1, keepdims=True)
    scaled = (tok_float * mix_gain).astype(bf16)
    weights = (w_query, w_key, w_decay, w_value, w_gate)
    partial = jnp.concatenate(
        [jnp.dot(scaled, w, preferred_element_type=f32) for w in weights]
        + [jnp.broadcast_to(squares, (squares.shape[0], 128))], axis=1).astype(bf16)
    blocks = [lax.dynamic_slice_in_dim(partial, (me ^ k) * seq_dev, seq_dev, 0) for k in range(kv_size)]
    projected = sum(b.astype(f32) for b in spread(blocks, kv_size, me))
    row_sums = projected[:, -1:]
    projected = projected * lax.rsqrt(row_sums / depth + epsilon)
    kw, vw = heads_here * key_dim, heads_here * val_dim
    queries = (projected[:, :kw] * key_dim ** (-0.5)).reshape(seq_dev, heads_here, key_dim)
    new_keys = projected[:, kw: 2 * kw].reshape(seq_dev, heads_here, key_dim)
    retain = jax.nn.sigmoid(projected[:, 2 * kw: 3 * kw] + decay_offset).reshape(seq_dev, heads_here, key_dim)
    values = projected[:, 3 * kw: 3 * kw + vw].reshape(seq_dev, heads_here, val_dim)
    gates = projected[:, 3 * kw + vw: 3 * kw + 2 * vw]
    new_state = retain[..., None] * state + new_keys[..., None] * values[:, :, None, :]
    readout = jnp.einsum("bhk,bhkv->bhv", queries, new_state, precision=lax.Precision.HIGHEST)
    readout = readout * lax.rsqrt(jnp.mean(readout * readout, axis=2, keepdims=True) + epsilon) * head_gain
    gated = (readout.reshape(seq_dev, vw) * jax.nn.silu(gates)).astype(bf16)

    arrived = spread([gated] * kv_size, kv_size, me)
    order = jnp.arange(kv_size) ^ me
    gated_all = jnp.take(jnp.stack(arrived), order, axis=0).reshape(kv_size * seq_dev, vw)
    branch = jnp.dot(gated_all, w_out, preferred_element_type=f32)
    branch_sent = branch.astype(bf16)
    branch_total = branch + swap_cores(branch_sent).astype(f32)
    stream_cols = (tok_float + branch_total).astype(bf16)
    stream_parts = spread([stream_cols] * kv_size, kv_size, me)
    stream = jnp.take(jnp.stack(stream_parts), order, axis=0)
    stream = stream.transpose(1, 0, 2).reshape(stream_cols.shape[0], depth)
    stream_float = stream.astype(f32)
    mlp_scale = lax.rsqrt(jnp.mean(stream_float * stream_float, axis=1, keepdims=True) + epsilon)
    normed = (stream_float * mlp_gain).astype(bf16)
    hidden = jnp.dot(normed, w_up, preferred_element_type=f32) * mlp_scale
    squared = jnp.square(jax.nn.relu(hidden)).astype(bf16)
    down = jnp.dot(squared, w_down, preferred_element_type=f32)
    rows = down.shape[0]
    down = down.reshape(rows, kv_size, 2, own_width)
    keep = jnp.where(core == 0, down[:, :, 0], down[:, :, 1])
    give = jnp.where(core == 0, down[:, :, 1], down[:, :, 0]).astype(bf16)
    pair = (keep + swap_cores(give).astype(f32)).astype(bf16)
    pieces = [lax.dynamic_index_in_dim(pair, me ^ k, 1, keepdims=False) for k in range(kv_size)]
    down_own = sum(p.astype(f32) for p in spread(pieces, kv_size, me))
    stream_own = lax.dynamic_slice_in_dim(stream_cols, core * own_width, own_width, 1)
    mixed = (stream_own.astype(f32) + down_own).astype(bf16)
    return (mixed, new_state)


def solution(mesh):
    kv_size = mesh.shape["kv"]
    in_specs = (
        P("dp", ("kv", "tp")),
        P(("dp", "kv"), "tp", None, None),
        P("kv"),
        P("kv", "tp"),
        P("kv", "tp"),
        P("kv", "tp"),
        P("kv", "tp"),
        P("kv", "tp"),
        P("tp"),
        P(),
        P("tp", "kv"),
        P(),
        P(None, ("kv", "tp")),
        P(("kv", "tp"), None),
    )
    out_specs = (P("dp", ("kv", "tp")), P(("dp", "kv"), "tp", None, None))

    def body(*args):
        return shards(kv_size, *args)

    return jax.shard_map(body, mesh=mesh, in_specs=in_specs, out_specs=out_specs, check_vma=False)
```

```python
import functools

import jax
import jax.numpy as jnp
from jax import lax
from jax.experimental import pallas as pl
from jax.experimental.pallas import tpu as pltpu
from jax.sharding import PartitionSpec as P


epsilon = 1e-06
bf16, f32 = jnp.bfloat16, jnp.float32
VMEM = pl.BlockSpec(memory_space=pltpu.VMEM)
HEAVY = pl.CostEstimate(flops=2 * 10**10, bytes_accessed=2**20, transcendentals=0)


def swap_cores(value):
    return lax.ppermute(value, "tp", [(0, 1), (1, 0)])


def spread(pieces, kv_size):
    came = []
    for k in range(1, kv_size):
        came.append(lax.ppermute(pieces[k], "kv", [(i, i ^ k) for i in range(kv_size)]))
    return [pieces[0]] + came


def here():
    return lax.axis_index("kv"), lax.axis_index("tp")


def aligned(start, step):
    return pl.multiple_of(start * step, step)


def clear_kernel(squares_ref):
    squares_ref[...] = jnp.zeros_like(squares_ref)


def project_kernel(squares_ref, own_ref, other_ref, gain_ref, *refs):
    *weights, total = refs
    weights, outs = weights[:5], weights[5:]
    count = len(outs)
    seqs = outs[0].shape[0]
    me, core = here()
    half = other_ref.shape[1]
    own, other = own_ref[...].astype(f32), other_ref[...].astype(f32)
    squares = squares_ref[...] + (
        jnp.sum(own * own, axis=1, keepdims=True) + jnp.sum(other * other, axis=1, keepdims=True))
    high = squares.astype(bf16).astype(f32)
    own_scaled = (own * gain_ref[:, pl.ds(aligned(core, half), half)]).astype(bf16)
    other_scaled = (other * gain_ref[:, pl.ds(aligned(1 - core, half), half)]).astype(bf16)
    own_rows, other_rows = pl.ds(aligned(core, half), half), pl.ds(aligned(1 - core, half), half)
    start = 0
    blocks = [
        jnp.dot(own_scaled, w[own_rows, :], preferred_element_type=f32)
        + jnp.dot(other_scaled, w[other_rows, :], preferred_element_type=f32)
        for w in weights
    ] + [high, squares - high]
    for block in blocks:
        for d in range(count):
            total[d, :, start: start + block.shape[1]] = block[d * seqs: (d + 1) * seqs]
        start += block.shape[1]
    for k, out in zip(range(count - 1, -1, -1), outs):
        out[...] = total[me ^ k].astype(out.dtype)


def project(squares, tokens, other, mix_gain, weights, kv_size):
    seqs = other.shape[0] // kv_size
    width = sum(w.shape[1] for w in weights) + 256
    outs = [jax.ShapeDtypeStruct((seqs, width), f32 if k == 0 else bf16) for k in range(kv_size - 1, -1, -1)]
    return pl.pallas_call(
        project_kernel,
        out_shape=outs,
        in_specs=[VMEM] * (4 + len(weights)),
        out_specs=[VMEM] * kv_size,
        scratch_shapes=[pltpu.VMEM((kv_size, seqs, width), f32)],
        compiler_params=pltpu.CompilerParams(vmem_limit_bytes=8 * 2**20),
        cost_estimate=HEAVY,
        name="project",
    )(squares, tokens, other, mix_gain.reshape(1, -1), *weights)[::-1]


def readout_kernel(kv_size, depth, *refs):
    parts = refs[:kv_size]
    state_ref, offset_ref, gain_ref, gated_ref, columns_ref, values_ref = refs[kv_size:]
    seqs, heads, keys, vals = state_ref.shape
    kw, vw = heads * keys, heads * vals
    base = 3 * kw + 2 * vw

    def summed(start, width):
        return sum(p[:, start: start + width].astype(f32) for p in parts)

    sums = summed(base, 128)[:, :1] + summed(base + 128, 128)[:, :1]
    row_scale = lax.rsqrt(sums / depth + epsilon)
    queries = summed(0, kw) * row_scale * keys ** (-0.5)
    new_keys = summed(kw, kw) * row_scale
    retain = jax.nn.sigmoid(summed(2 * kw, kw) * row_scale + offset_ref[...])
    values = summed(3 * kw, vw) * row_scale
    gates = summed(3 * kw + vw, vw) * row_scale
    values_ref[...] = values
    fill = jnp.zeros((-3 * seqs % 8, kw), f32)
    columns = jnp.concatenate([queries * retain, retain, new_keys] + ([fill] if fill.shape[0] else []), axis=0).T
    columns_ref[...] = columns
    silu = gates * jax.nn.sigmoid(gates)
    for h in range(heads):
        qk = jnp.sum(queries[:, h * keys: (h + 1) * keys] * new_keys[:, h * keys: (h + 1) * keys], axis=1,
                     keepdims=True)
        reads = []
        for b in range(seqs):
            weight = columns[h * keys: (h + 1) * keys, b: b + 1]
            reads.append(jnp.sum(weight * state_ref[b, h], axis=0, keepdims=True))
        read = jnp.concatenate(reads, axis=0) + qk * values[:, h * vals: (h + 1) * vals]
        read = read * lax.rsqrt(jnp.mean(read * read, axis=1, keepdims=True) + epsilon) * gain_ref[...]
        gated_ref[:, h * vals: (h + 1) * vals] = (read * silu[:, h * vals: (h + 1) * vals]).astype(bf16)


def readout(parts, state, decay_offset, head_gain, depth):
    seqs, heads, keys, vals = state.shape
    height = 3 * seqs + (-3 * seqs % 8)
    outs = [
        jax.ShapeDtypeStruct((seqs, heads * vals), bf16),
        jax.ShapeDtypeStruct((heads * keys, height), f32),
        jax.ShapeDtypeStruct((seqs, heads * vals), f32),
    ]
    return pl.pallas_call(
        functools.partial(readout_kernel, len(parts), depth),
        out_shape=outs,
        in_specs=[VMEM] * (len(parts) + 3),
        out_specs=[VMEM] * 3,
        compiler_params=pltpu.CompilerParams(vmem_limit_bytes=12 * 2**20),
        cost_estimate=HEAVY,
        name="readout",
    )(*parts, state, decay_offset.reshape(1, -1), head_gain.reshape(1, -1))


def update_kernel(columns_ref, values_ref, state_ref, out_ref):
    seqs = values_ref.shape[0]
    b, h = pl.program_id(0), pl.program_id(1)
    keys, vals = out_ref.shape[2:]
    block = columns_ref[pl.ds(aligned(h, keys), keys), :]
    lanes = lax.broadcasted_iota(jnp.int32, (1, block.shape[1]), 1)
    keep = jnp.sum(jnp.where(lanes == seqs + b, block, 0.0), axis=1, keepdims=True)
    key = jnp.sum(jnp.where(lanes == 2 * seqs + b, block, 0.0), axis=1, keepdims=True)
    value = values_ref[pl.ds(b, 1), pl.ds(aligned(h, vals), vals)]
    out_ref[0, 0] = keep * state_ref[0, 0] + key * value


def update(columns, values, state):
    seqs, heads, keys, vals = state.shape
    tile = pl.BlockSpec((1, 1, keys, vals), lambda b, h: (b, h, 0, 0))
    return pl.pallas_call(
        update_kernel,
        out_shape=jax.ShapeDtypeStruct(state.shape, f32),
        grid=(seqs, heads),
        in_specs=[VMEM, VMEM, tile],
        out_specs=tile,
        compiler_params=pltpu.CompilerParams(vmem_limit_bytes=8 * 2**20),
        cost_estimate=HEAVY,
        name="update",
    )(columns, values, state)


def branch_kernel(*refs):
    *parts, w_ref, keep_ref, send_ref, rows = refs
    me, _ = here()
    for k, part in enumerate(parts):
        rows[me ^ k] = part[...].astype(f32)
    gated = jnp.concatenate([rows[d] for d in range(len(parts))], axis=0).astype(bf16)
    branch = jnp.dot(gated, w_ref[...], preferred_element_type=f32)
    keep_ref[...] = branch
    send_ref[...] = branch.astype(bf16)


def branch_of(parts, w_out):
    rows = parts[0].shape[0] * len(parts)
    outs = [jax.ShapeDtypeStruct((rows, w_out.shape[1]), kind) for kind in (f32, bf16)]
    return pl.pallas_call(
        branch_kernel,
        out_shape=outs,
        in_specs=[VMEM] * (len(parts) + 1),
        out_specs=[VMEM] * 2,
        scratch_shapes=[pltpu.VMEM((len(parts), *parts[0].shape), f32)],
        compiler_params=pltpu.CompilerParams(vmem_limit_bytes=4 * 2**20),
        cost_estimate=HEAVY,
        name="branch",
    )(*parts, w_out)


def mixer_kernel(*refs):
    *parts, gain_ref, up_ref, down_ref, keep_ref, give_ref, total = refs
    me, core = here()
    width = parts[0].shape[1]
    depth = width * len(parts)
    own = width // 2
    squares, hidden = 0.0, 0.0
    for k, part in enumerate(parts):
        owner = me ^ k
        stream = part[...].astype(f32)
        squares += jnp.sum(stream * stream, axis=1, keepdims=True)
        normed = (stream * gain_ref[:, pl.ds(aligned(owner, width), width)]).astype(bf16)
        hidden += jnp.dot(normed, up_ref[pl.ds(aligned(owner, width), width), :], preferred_element_type=f32)
    hidden = hidden * lax.rsqrt(squares / depth + epsilon)
    squared = jnp.square(jnp.maximum(hidden, 0.0)).astype(bf16)
    total[...] = jnp.dot(squared, down_ref[...], preferred_element_type=f32)
    for d in range(len(parts)):
        keep_ref[d] = total[:, pl.ds(aligned(2 * d + core, own), own)]
        give_ref[d] = total[:, pl.ds(aligned(2 * d + 1 - core, own), own)].astype(bf16)


def mixer(parts, mlp_gain, w_up, w_down):
    rows, width = parts[0].shape
    outs = [jax.ShapeDtypeStruct((len(parts), rows, width // 2), kind) for kind in (f32, bf16)]
    return pl.pallas_call(
        mixer_kernel,
        out_shape=outs,
        in_specs=[VMEM] * (len(parts) + 3),
        out_specs=[VMEM] * 2,
        scratch_shapes=[pltpu.VMEM((rows, w_down.shape[1]), f32)],
        compiler_params=pltpu.CompilerParams(vmem_limit_bytes=16 * 2**20),
        cost_estimate=HEAVY,
        name="mixer",
    )(*parts, mlp_gain.reshape(1, -1), w_up, w_down)


def stream_kernel(branch_ref, came_ref, own_ref, other_ref, stream_ref):
    _, core = here()
    half = own_ref.shape[1]
    for ref, side in ((own_ref, core), (other_ref, 1 - core)):
        at = pl.ds(aligned(side, half), half)
        total = branch_ref[:, at] + came_ref[:, at].astype(f32)
        stream_ref[:, at] = (ref[...].astype(f32) + total).astype(bf16)


def pair_kernel(keep_ref, came_ref, *outs):
    me, _ = here()
    for k, out in zip(range(len(outs) - 1, -1, -1), outs):
        out[...] = (keep_ref[me ^ k] + came_ref[me ^ k].astype(f32)).astype(out.dtype)


def last_kernel(stream_ref, *refs):
    *parts, out_ref = refs
    _, core = here()
    half = out_ref.shape[1]
    total = sum(p[...].astype(f32) for p in parts)
    out_ref[...] = (stream_ref[:, pl.ds(aligned(core, half), half)].astype(f32) + total).astype(bf16)


def small(body, outs, *args):
    return pl.pallas_call(
        body,
        out_shape=outs,
        in_specs=[VMEM] * len(args),
        out_specs=jax.tree.map(lambda _: VMEM, outs),
        compiler_params=pltpu.CompilerParams(vmem_limit_bytes=2 * 2**20),
        cost_estimate=HEAVY,
    )(*args)


def fused_steps(kv_size, tokens, state, mix_gain, weights, decay_offset, head_gain, w_out, mlp_gain, w_up, w_down):
    rows, half = tokens.shape
    depth = 2 * half * kv_size
    like = jax.ShapeDtypeStruct
    other = swap_cores(tokens)
    squares = small(clear_kernel, like((rows, 128), f32))
    parts = spread(project(squares, tokens, other, mix_gain, weights, kv_size), kv_size)
    gated, columns, values = readout(parts, state, decay_offset, head_gain, depth)
    arrived = spread([gated] * kv_size, kv_size)
    new_state = update(columns, values, state)
    branch, branch_sent = branch_of(arrived, w_out)
    stream = small(stream_kernel, like((rows, 2 * half), bf16), branch, swap_cores(branch_sent), tokens, other)
    keep, give = mixer(spread([stream] * kv_size, kv_size), mlp_gain, w_up, w_down)
    outs = [like((rows, half), f32 if k == 0 else bf16) for k in range(kv_size - 1, -1, -1)]
    pieces = spread(small(pair_kernel, outs, keep, swap_cores(give))[::-1], kv_size)
    return small(last_kernel, like((rows, half), bf16), stream, *pieces), new_state


def plain_steps(kv_size, tokens, state, mix_gain, weights, decay_offset, head_gain, w_out, mlp_gain, w_up, w_down):
    seqs, heads, keys, vals = state.shape
    rows, half = tokens.shape
    depth = 2 * half * kv_size
    core = lax.axis_index("tp")

    def exchange(blocks):
        return lax.all_to_all(blocks, "kv", 0, 0, tiled=True)

    def pick(pair):
        return jnp.where(core == 0, pair[0], pair[1]), jnp.where(core == 0, pair[1], pair[0])

    other = swap_cores(tokens)
    tok = jnp.concatenate(pick((tokens, other)), axis=1).astype(f32)
    squares = jnp.sum(tok * tok, axis=1, keepdims=True)
    scaled = (tok * mix_gain).astype(bf16)
    high = squares.astype(bf16).astype(f32)
    total = jnp.concatenate([jnp.dot(scaled, w, preferred_element_type=f32) for w in weights]
                            + [jnp.broadcast_to(x, (rows, 128)) for x in (high, squares - high)], axis=1)
    came = exchange(total.astype(bf16).reshape(kv_size, seqs, -1))
    total = jnp.sum(came.astype(f32), axis=0)
    kw, vw = heads * keys, heads * vals
    sums = total[:, 3 * kw + 2 * vw] + total[:, 3 * kw + 2 * vw + 128]
    total = total * lax.rsqrt(sums / depth + epsilon)[:, None]
    queries = (total[:, :kw] * keys ** (-0.5)).reshape(seqs, heads, keys)
    new_keys = total[:, kw: 2 * kw].reshape(seqs, heads, keys)
    retain = jax.nn.sigmoid(total[:, 2 * kw: 3 * kw] + decay_offset).reshape(seqs, heads, keys)
    values = total[:, 3 * kw: 3 * kw + vw].reshape(seqs, heads, vals)
    gates = total[:, 3 * kw + vw: 3 * kw + 2 * vw]
    new_state = retain[..., None] * state + new_keys[..., None] * values[:, :, None, :]
    read = jnp.einsum("bhk,bhkv->bhv", queries, new_state, precision=lax.Precision.HIGHEST)
    read = read * lax.rsqrt(jnp.mean(read * read, axis=2, keepdims=True) + epsilon) * head_gain
    gated = (read.reshape(seqs, vw) * jax.nn.silu(gates)).astype(bf16)
    gated = lax.all_gather(gated, "kv", axis=0, tiled=True)
    branch = jnp.dot(gated, w_out, preferred_element_type=f32)
    branch = branch + swap_cores(branch.astype(bf16)).astype(f32)
    stream_cols = (tok + branch).astype(bf16)
    stream = lax.all_gather(stream_cols, "kv", axis=1, tiled=True).astype(f32)
    scale = lax.rsqrt(jnp.mean(stream * stream, axis=1, keepdims=True) + epsilon)
    normed = (stream * mlp_gain).astype(bf16)
    hidden = jnp.dot(normed, w_up, preferred_element_type=f32) * scale
    squared = jnp.square(jax.nn.relu(hidden)).astype(bf16)
    down = jnp.dot(squared, w_down, preferred_element_type=f32)
    keep, give = pick(down.reshape(rows, kv_size, 2, half).transpose(2, 1, 0, 3))
    pair = keep + swap_cores(give.astype(bf16)).astype(f32)
    down_own = jnp.sum(exchange(pair.astype(bf16)).astype(f32), axis=0)
    stream_own, _ = pick((stream_cols[:, :half], stream_cols[:, half:]))
    return (stream_own.astype(f32) + down_own).astype(bf16), new_state


def shards(kv_size, tokens, state, mix_gain, w_query, w_key, w_decay, w_value, w_gate, *rest):
    steps = fused_steps if tokens.shape[1] % 128 == 0 and kv_size in (2, 4, 8) else plain_steps
    return steps(kv_size, tokens, state, mix_gain, (w_query, w_key, w_decay, w_value, w_gate), *rest)


def solution(mesh):
    kv_size = mesh.shape["kv"]
    in_specs = (
        P("dp", ("kv", "tp")),
        P(("dp", "kv"), "tp", None, None),
        P("kv"),
        P("kv", "tp"),
        P("kv", "tp"),
        P("kv", "tp"),
        P("kv", "tp"),
        P("kv", "tp"),
        P("tp"),
        P(),
        P("tp", "kv"),
        P(),
        P(None, ("kv", "tp")),
        P(("kv", "tp"), None),
    )
    out_specs = (P("dp", ("kv", "tp")), P(("dp", "kv"), "tp", None, None))

    def body(*args):
        return shards(kv_size, *args)

    return jax.shard_map(body, mesh=mesh, in_specs=in_specs, out_specs=out_specs, check_vma=False)
```

```python
import functools

import jax
import jax.numpy as jnp
from jax import lax
from jax.experimental import pallas as pl
from jax.experimental.pallas import tpu as pltpu
from jax.sharding import PartitionSpec as P


epsilon = 1e-06
bf16, f32 = jnp.bfloat16, jnp.float32
VMEM = pl.BlockSpec(memory_space=pltpu.VMEM)
HEAVY = pl.CostEstimate(flops=2 * 10**10, bytes_accessed=2**20, transcendentals=0)


def swap_cores(value):
    return lax.ppermute(value, "tp", [(0, 1), (1, 0)])


def spread(pieces, kv_size, cross):
    came = []
    for k in range(1, kv_size):
        pairs = [(2 * i + c, 2 * (i ^ k) + (c ^ cross)) for i in range(kv_size) for c in (0, 1)]
        came.append(lax.ppermute(pieces[k], ("kv", "tp"), pairs))
    return [pieces[0]] + came


def here():
    return lax.axis_index("kv"), lax.axis_index("tp")


def aligned(start, step):
    return pl.multiple_of(start * step, step)


def clear_kernel(squares_ref):
    squares_ref[...] = jnp.zeros_like(squares_ref)


def project_kernel(squares_ref, own_ref, other_ref, gain_ref, *refs):
    *weights, total = refs
    weights, outs = weights[:5], weights[5:]
    count = len(outs)
    seqs = outs[0].shape[0]
    me, core = here()
    half = other_ref.shape[1]
    own, other = own_ref[...].astype(f32), other_ref[...].astype(f32)
    squares = squares_ref[...] + (
        jnp.sum(own * own, axis=1, keepdims=True) + jnp.sum(other * other, axis=1, keepdims=True))
    high = squares.astype(bf16).astype(f32)
    own_scaled = (own * gain_ref[:, pl.ds(aligned(core, half), half)]).astype(bf16)
    other_scaled = (other * gain_ref[:, pl.ds(aligned(1 - core, half), half)]).astype(bf16)
    own_rows, other_rows = pl.ds(aligned(core, half), half), pl.ds(aligned(1 - core, half), half)
    start = 0
    blocks = [
        jnp.dot(own_scaled, w[own_rows, :], preferred_element_type=f32)
        + jnp.dot(other_scaled, w[other_rows, :], preferred_element_type=f32)
        for w in weights
    ] + [high, squares - high]
    for block in blocks:
        for d in range(count):
            total[d, :, start: start + block.shape[1]] = block[d * seqs: (d + 1) * seqs]
        start += block.shape[1]
    for k, out in zip(range(count - 1, -1, -1), outs):
        out[...] = total[me ^ k].astype(out.dtype)


def project(squares, tokens, other, mix_gain, weights, kv_size):
    seqs = other.shape[0] // kv_size
    width = sum(w.shape[1] for w in weights) + 256
    outs = [jax.ShapeDtypeStruct((seqs, width), f32 if k == 0 else bf16) for k in range(kv_size - 1, -1, -1)]
    return pl.pallas_call(
        project_kernel,
        out_shape=outs,
        in_specs=[VMEM] * (4 + len(weights)),
        out_specs=[VMEM] * kv_size,
        scratch_shapes=[pltpu.VMEM((kv_size, seqs, width), f32)],
        compiler_params=pltpu.CompilerParams(vmem_limit_bytes=8 * 2**20),
        cost_estimate=HEAVY,
        name="project",
    )(squares, tokens, other, mix_gain.reshape(1, -1), *weights)[::-1]


def readout_kernel(kv_size, depth, *refs):
    parts = refs[:kv_size]
    state_ref, offset_ref, gain_ref, gated_ref, columns_ref, values_ref = refs[kv_size:]
    seqs, heads, keys, vals = state_ref.shape
    kw, vw = heads * keys, heads * vals
    base = 3 * kw + 2 * vw

    def summed(start, width):
        return sum(p[:, start: start + width].astype(f32) for p in parts)

    sums = summed(base, 128)[:, :1] + summed(base + 128, 128)[:, :1]
    row_scale = lax.rsqrt(sums / depth + epsilon)
    queries = summed(0, kw) * row_scale * keys ** (-0.5)
    new_keys = summed(kw, kw) * row_scale
    retain = jax.nn.sigmoid(summed(2 * kw, kw) * row_scale + offset_ref[...])
    values = summed(3 * kw, vw) * row_scale
    gates = summed(3 * kw + vw, vw) * row_scale
    values_ref[...] = values
    fill = jnp.zeros((-3 * seqs % 8, kw), f32)
    columns = jnp.concatenate([queries * retain, retain, new_keys] + ([fill] if fill.shape[0] else []), axis=0).T
    columns_ref[...] = columns
    silu = gates * jax.nn.sigmoid(gates)
    for h in range(heads):
        qk = jnp.sum(queries[:, h * keys: (h + 1) * keys] * new_keys[:, h * keys: (h + 1) * keys], axis=1,
                     keepdims=True)
        reads = []
        for b in range(seqs):
            weight = columns[h * keys: (h + 1) * keys, b: b + 1]
            reads.append(jnp.sum(weight * state_ref[b, h], axis=0, keepdims=True))
        read = jnp.concatenate(reads, axis=0) + qk * values[:, h * vals: (h + 1) * vals]
        read = read * lax.rsqrt(jnp.mean(read * read, axis=1, keepdims=True) + epsilon) * gain_ref[...]
        gated_ref[:, h * vals: (h + 1) * vals] = (read * silu[:, h * vals: (h + 1) * vals]).astype(bf16)


def readout(parts, state, decay_offset, head_gain, depth):
    seqs, heads, keys, vals = state.shape
    height = 3 * seqs + (-3 * seqs % 8)
    outs = [
        jax.ShapeDtypeStruct((seqs, heads * vals), bf16),
        jax.ShapeDtypeStruct((heads * keys, height), f32),
        jax.ShapeDtypeStruct((seqs, heads * vals), f32),
    ]
    return pl.pallas_call(
        functools.partial(readout_kernel, len(parts), depth),
        out_shape=outs,
        in_specs=[VMEM] * (len(parts) + 3),
        out_specs=[VMEM] * 3,
        compiler_params=pltpu.CompilerParams(vmem_limit_bytes=12 * 2**20),
        cost_estimate=HEAVY,
        name="readout",
    )(*parts, state, decay_offset.reshape(1, -1), head_gain.reshape(1, -1))


def update_kernel(first, count, columns_ref, values_ref, state_ref, *refs):
    out_hbm, tiles, sems = refs[-3:]
    seqs, heads, keys, vals = state_ref.shape
    copies = []
    for n in range(count):
        b = first + n
        for h in range(heads):
            rows = slice(h * keys, (h + 1) * keys)
            keep = columns_ref[rows, seqs + b: seqs + b + 1]
            key = columns_ref[rows, 2 * seqs + b: 2 * seqs + b + 1]
            value = values_ref[b: b + 1, h * vals: (h + 1) * vals]
            tiles[n, h] = keep * state_ref[b, h] + key * value
            copies.append(pltpu.make_async_copy(tiles.at[n, h], out_hbm.at[b, h], sems.at[n, h]))
            copies[-1].start()
    for copy in copies:
        copy.wait()


def update(columns, values, state, first, count, *written):
    return pl.pallas_call(
        functools.partial(update_kernel, first, count),
        out_shape=jax.ShapeDtypeStruct(state.shape, f32),
        in_specs=[VMEM, VMEM, VMEM] + [pl.BlockSpec(memory_space=pl.ANY)] * len(written),
        out_specs=pl.BlockSpec(memory_space=pl.ANY),
        scratch_shapes=[pltpu.VMEM((count, *state.shape[1:]), f32), pltpu.SemaphoreType.DMA((count, state.shape[1]))],
        input_output_aliases={3: 0} if written else {},
        compiler_params=pltpu.CompilerParams(vmem_limit_bytes=8 * 2**20),
        cost_estimate=HEAVY,
        name="update",
    )(columns, values, state, *written)


def branch_kernel(*refs):
    *parts, own_w, other_w, keep_ref, send_ref, rows = refs
    me, _ = here()
    count, seqs = len(parts), parts[0].shape[0]
    pad = [jnp.zeros((-seqs % 8, parts[0].shape[1]), f32)] if seqs % 8 else []
    own = jnp.concatenate([parts[0][...].astype(f32)] + pad, axis=0).astype(bf16)
    far = jnp.concatenate([part[...].astype(f32) for part in parts[1:]] + [parts[0][...].astype(f32)], axis=0)
    own = jnp.dot(own, own_w[...], preferred_element_type=f32)
    far = jnp.dot(far.astype(bf16), other_w[...], preferred_element_type=f32)
    rows[me] = own[:seqs]
    for k in range(1, count):
        rows[me ^ k] = far[(k - 1) * seqs: k * seqs]
    for d in range(count):
        keep_ref[d * seqs: (d + 1) * seqs, :] = rows[d]
    send_ref[...] = keep_ref[...].astype(bf16)


def branch_of(parts, own_w, other_w):
    rows = parts[0].shape[0] * len(parts)
    outs = [jax.ShapeDtypeStruct((rows, own_w.shape[1]), kind) for kind in (f32, bf16)]
    return pl.pallas_call(
        branch_kernel,
        out_shape=outs,
        in_specs=[VMEM] * (len(parts) + 2),
        out_specs=[VMEM] * 2,
        scratch_shapes=[pltpu.VMEM((len(parts), parts[0].shape[0], own_w.shape[1]), f32)],
        compiler_params=pltpu.CompilerParams(vmem_limit_bytes=4 * 2**20),
        cost_estimate=HEAVY,
        name="branch",
    )(*parts, own_w, other_w)


def mixer_kernel(*refs):
    *parts, gain_ref, up_ref, down_ref, keep_ref, give_ref, total = refs
    me, core = here()
    width = parts[0].shape[1]
    depth = width * len(parts)
    own = width // 2
    squares, hidden = 0.0, 0.0
    for k, part in enumerate(parts):
        owner = me ^ k
        stream = part[...].astype(f32)
        squares += jnp.sum(stream * stream, axis=1, keepdims=True)
        normed = (stream * gain_ref[:, pl.ds(aligned(owner, width), width)]).astype(bf16)
        hidden += jnp.dot(normed, up_ref[pl.ds(aligned(owner, width), width), :], preferred_element_type=f32)
    hidden = hidden * lax.rsqrt(squares / depth + epsilon)
    squared = jnp.square(jnp.maximum(hidden, 0.0)).astype(bf16)
    total[...] = jnp.dot(squared, down_ref[...], preferred_element_type=f32)
    for k in range(len(parts)):
        side = core if k == 0 else 1 - core
        keep_ref[k] = total[:, pl.ds(aligned(2 * (me ^ k) + side, own), own)]
        give_ref[k] = total[:, pl.ds(aligned(2 * (me ^ k) + 1 - side, own), own)].astype(bf16)


def mixer(parts, mlp_gain, w_up, w_down):
    rows, width = parts[0].shape
    outs = [jax.ShapeDtypeStruct((len(parts), rows, width // 2), kind) for kind in (f32, bf16)]
    return pl.pallas_call(
        mixer_kernel,
        out_shape=outs,
        in_specs=[VMEM] * (len(parts) + 3),
        out_specs=[VMEM] * 2,
        scratch_shapes=[pltpu.VMEM((rows, w_down.shape[1]), f32)],
        compiler_params=pltpu.CompilerParams(vmem_limit_bytes=16 * 2**20),
        cost_estimate=HEAVY,
        name="mixer",
    )(*parts, mlp_gain.reshape(1, -1), w_up, w_down)


def stream_kernel(branch_ref, came_ref, own_ref, other_ref, stream_ref):
    _, core = here()
    half = own_ref.shape[1]
    for ref, side in ((own_ref, core), (other_ref, 1 - core)):
        at = pl.ds(aligned(side, half), half)
        total = branch_ref[:, at] + came_ref[:, at].astype(f32)
        stream_ref[:, at] = (ref[...].astype(f32) + total).astype(bf16)


def pair_kernel(keep_ref, came_ref, *outs):
    for k, out in zip(range(len(outs) - 1, -1, -1), outs):
        out[...] = (keep_ref[k] + came_ref[k].astype(f32)).astype(out.dtype)


def last_kernel(stream_ref, *refs):
    *parts, out_ref = refs
    _, core = here()
    half = out_ref.shape[1]
    total = sum(p[...].astype(f32) for p in parts)
    out_ref[...] = (stream_ref[:, pl.ds(aligned(core, half), half)].astype(f32) + total).astype(bf16)


def small(body, outs, *args):
    return pl.pallas_call(
        body,
        out_shape=outs,
        in_specs=[VMEM] * len(args),
        out_specs=jax.tree.map(lambda _: VMEM, outs),
        compiler_params=pltpu.CompilerParams(vmem_limit_bytes=2 * 2**20),
        cost_estimate=HEAVY,
    )(*args)


def fused_steps(kv_size, tokens, state, mix_gain, weights, decay_offset, head_gain, w_out, mlp_gain, w_up, w_down):
    rows, half = tokens.shape
    depth = 2 * half * kv_size
    like = jax.ShapeDtypeStruct
    other = swap_cores(tokens)
    squares = small(clear_kernel, like((rows, 128), f32))
    parts = spread(project(squares, tokens, other, mix_gain, weights, kv_size), kv_size, 0)
    gated, columns, values = readout(parts, state, decay_offset, head_gain, depth)
    arrived = spread([gated] * kv_size, kv_size, 1)
    new_state = update(columns, values, state, 0, 2)
    new_state = update(columns, values, state, 2, 2, new_state)
    w_other = swap_cores(w_out)
    branch, branch_sent = branch_of(arrived, w_out, w_other)
    stream = small(stream_kernel, like((rows, 2 * half), bf16), branch, swap_cores(branch_sent), tokens, other)
    keep, give = mixer(spread([stream] * kv_size, kv_size, 1), mlp_gain, w_up, w_down)
    outs = [like((rows, half), f32 if k == 0 else bf16) for k in range(kv_size - 1, -1, -1)]
    pieces = spread(small(pair_kernel, outs, keep, swap_cores(give))[::-1], kv_size, 1)
    return small(last_kernel, like((rows, half), bf16), stream, *pieces), new_state


def plain_steps(kv_size, tokens, state, mix_gain, weights, decay_offset, head_gain, w_out, mlp_gain, w_up, w_down):
    seqs, heads, keys, vals = state.shape
    rows, half = tokens.shape
    depth = 2 * half * kv_size
    core = lax.axis_index("tp")

    def exchange(blocks):
        return lax.all_to_all(blocks, "kv", 0, 0, tiled=True)

    def pick(pair):
        return jnp.where(core == 0, pair[0], pair[1]), jnp.where(core == 0, pair[1], pair[0])

    other = swap_cores(tokens)
    tok = jnp.concatenate(pick((tokens, other)), axis=1).astype(f32)
    squares = jnp.sum(tok * tok, axis=1, keepdims=True)
    scaled = (tok * mix_gain).astype(bf16)
    high = squares.astype(bf16).astype(f32)
    total = jnp.concatenate([jnp.dot(scaled, w, preferred_element_type=f32) for w in weights]
                            + [jnp.broadcast_to(x, (rows, 128)) for x in (high, squares - high)], axis=1)
    came = exchange(total.astype(bf16).reshape(kv_size, seqs, -1))
    total = jnp.sum(came.astype(f32), axis=0)
    kw, vw = heads * keys, heads * vals
    sums = total[:, 3 * kw + 2 * vw] + total[:, 3 * kw + 2 * vw + 128]
    total = total * lax.rsqrt(sums / depth + epsilon)[:, None]
    queries = (total[:, :kw] * keys ** (-0.5)).reshape(seqs, heads, keys)
    new_keys = total[:, kw: 2 * kw].reshape(seqs, heads, keys)
    retain = jax.nn.sigmoid(total[:, 2 * kw: 3 * kw] + decay_offset).reshape(seqs, heads, keys)
    values = total[:, 3 * kw: 3 * kw + vw].reshape(seqs, heads, vals)
    gates = total[:, 3 * kw + vw: 3 * kw + 2 * vw]
    new_state = retain[..., None] * state + new_keys[..., None] * values[:, :, None, :]
    read = jnp.einsum("bhk,bhkv->bhv", queries, new_state, precision=lax.Precision.HIGHEST)
    read = read * lax.rsqrt(jnp.mean(read * read, axis=2, keepdims=True) + epsilon) * head_gain
    gated = (read.reshape(seqs, vw) * jax.nn.silu(gates)).astype(bf16)
    gated = lax.all_gather(gated, "kv", axis=0, tiled=True)
    branch = jnp.dot(gated, w_out, preferred_element_type=f32)
    branch = branch + swap_cores(branch.astype(bf16)).astype(f32)
    stream_cols = (tok + branch).astype(bf16)
    stream = lax.all_gather(stream_cols, "kv", axis=1, tiled=True).astype(f32)
    scale = lax.rsqrt(jnp.mean(stream * stream, axis=1, keepdims=True) + epsilon)
    normed = (stream * mlp_gain).astype(bf16)
    hidden = jnp.dot(normed, w_up, preferred_element_type=f32) * scale
    squared = jnp.square(jax.nn.relu(hidden)).astype(bf16)
    down = jnp.dot(squared, w_down, preferred_element_type=f32)
    keep, give = pick(down.reshape(rows, kv_size, 2, half).transpose(2, 1, 0, 3))
    pair = keep + swap_cores(give.astype(bf16)).astype(f32)
    down_own = jnp.sum(exchange(pair.astype(bf16)).astype(f32), axis=0)
    stream_own, _ = pick((stream_cols[:, :half], stream_cols[:, half:]))
    return (stream_own.astype(f32) + down_own).astype(bf16), new_state


def shards(kv_size, tokens, state, mix_gain, w_query, w_key, w_decay, w_value, w_gate, *rest):
    steps = fused_steps if tokens.shape[1] % 128 == 0 and kv_size in (2, 4, 8) else plain_steps
    return steps(kv_size, tokens, state, mix_gain, (w_query, w_key, w_decay, w_value, w_gate), *rest)


def solution(mesh):
    kv_size = mesh.shape["kv"]
    in_specs = (
        P("dp", ("kv", "tp")),
        P(("dp", "kv"), "tp", None, None),
        P("kv"),
        P("kv", "tp"),
        P("kv", "tp"),
        P("kv", "tp"),
        P("kv", "tp"),
        P("kv", "tp"),
        P("tp"),
        P(),
        P("tp", "kv"),
        P(),
        P(None, ("kv", "tp")),
        P(("kv", "tp"), None),
    )
    out_specs = (P("dp", ("kv", "tp")), P(("dp", "kv"), "tp", None, None))

    def body(*args):
        return shards(kv_size, *args)

    return jax.shard_map(body, mesh=mesh, in_specs=in_specs, out_specs=out_specs, check_vma=False)
```

```python
import functools

import jax
import jax.numpy as jnp
from jax import lax
from jax.experimental import pallas as pl
from jax.experimental.pallas import tpu as pltpu
from jax.sharding import PartitionSpec as P


epsilon = 1e-06
bf16, f32 = jnp.bfloat16, jnp.float32
VMEM = pl.BlockSpec(memory_space=pltpu.VMEM)
HEAVY = pl.CostEstimate(flops=2 * 10**10, bytes_accessed=2**20, transcendentals=0)
LIGHT = pl.CostEstimate(flops=2**17, bytes_accessed=2**17, transcendentals=0)


def swap_cores(value):
    return lax.ppermute(value, "tp", [(0, 1), (1, 0)])


def spread(pieces, kv_size, cross):
    came = []
    for k in range(1, kv_size):
        pairs = [(2 * i + c, 2 * (i ^ k) + (c ^ cross)) for i in range(kv_size) for c in (0, 1)]
        came.append(lax.ppermute(pieces[k], ("kv", "tp"), pairs))
    return [pieces[0]] + came


def here():
    return lax.axis_index("kv"), lax.axis_index("tp")


def aligned(start, step):
    return pl.multiple_of(start * step, step)


def clear_kernel(squares_ref):
    squares_ref[...] = jnp.zeros_like(squares_ref)


def project_kernel(squares_ref, own_ref, other_ref, gain_ref, *refs):
    *weights, total = refs
    weights, outs = weights[:5], weights[5:]
    count = len(outs)
    seqs = outs[0].shape[0]
    me, core = here()
    half = other_ref.shape[1]
    own, other = own_ref[...].astype(f32), other_ref[...].astype(f32)
    squares = squares_ref[...] + (
        jnp.sum(own * own, axis=1, keepdims=True) + jnp.sum(other * other, axis=1, keepdims=True))
    high = squares.astype(bf16).astype(f32)
    own_scaled = (own * gain_ref[:, pl.ds(aligned(core, half), half)]).astype(bf16)
    other_scaled = (other * gain_ref[:, pl.ds(aligned(1 - core, half), half)]).astype(bf16)
    own_rows, other_rows = pl.ds(aligned(core, half), half), pl.ds(aligned(1 - core, half), half)
    start = 0
    blocks = [
        jnp.dot(own_scaled, w[own_rows, :], preferred_element_type=f32)
        + jnp.dot(other_scaled, w[other_rows, :], preferred_element_type=f32)
        for w in weights
    ] + [high, squares - high]
    for block in blocks:
        for d in range(count):
            total[d, :, start: start + block.shape[1]] = block[d * seqs: (d + 1) * seqs]
        start += block.shape[1]
    for k, out in zip(range(count - 1, -1, -1), outs):
        out[...] = total[me ^ k].astype(out.dtype)


def project(squares, tokens, other, mix_gain, weights, kv_size):
    seqs = other.shape[0] // kv_size
    width = sum(w.shape[1] for w in weights) + 256
    outs = [jax.ShapeDtypeStruct((seqs, width), f32 if k == 0 else bf16) for k in range(kv_size - 1, -1, -1)]
    return pl.pallas_call(
        project_kernel,
        out_shape=outs,
        in_specs=[VMEM] * (4 + len(weights)),
        out_specs=[VMEM] * kv_size,
        scratch_shapes=[pltpu.VMEM((kv_size, seqs, width), f32)],
        compiler_params=pltpu.CompilerParams(vmem_limit_bytes=8 * 2**20),
        cost_estimate=HEAVY,
        name="project",
    )(squares, tokens, other, mix_gain.reshape(1, -1), *weights)[::-1]


def narrow_kernel(state_ref, out_ref):
    out_ref[...] = state_ref[...].astype(bf16)


def narrow(state):
    return pl.pallas_call(
        narrow_kernel,
        out_shape=jax.ShapeDtypeStruct(state.shape, bf16),
        in_specs=[VMEM],
        out_specs=VMEM,
        compiler_params=pltpu.CompilerParams(vmem_limit_bytes=8 * 2**20),
        cost_estimate=LIGHT,
        name="narrow",
    )(state)


def readout_kernel(kv_size, depth, *refs):
    parts = refs[:kv_size]
    state_ref, offset_ref, gain_ref, gated_ref, factors_ref, values_ref = refs[kv_size:]
    seqs, heads, keys, vals = state_ref.shape
    kw, vw = heads * keys, heads * vals

    def summed(start, width):
        return sum(p[:, start: start + width].astype(f32) for p in parts)

    base = 3 * kw + 2 * vw
    sums = summed(base, 128)[:, :1] + summed(base + 128, 128)[:, :1]
    row_scale = lax.rsqrt(sums / depth + epsilon)
    queries = summed(0, kw) * row_scale * keys ** (-0.5)
    new_keys = summed(kw, kw) * row_scale
    retain = jax.nn.sigmoid(summed(2 * kw, kw) * row_scale + offset_ref[...])
    kept = (queries * retain).astype(bf16)
    row = lax.broadcasted_iota(jnp.int32, (seqs, 1), 0)
    reads = []
    for h in range(heads):
        at = slice(h * keys, (h + 1) * keys)
        read = 0.0
        for b in range(seqs):
            product = jnp.dot(kept[:, at], state_ref[b, h], preferred_element_type=f32)
            read += jnp.where(row == b, product, 0.0)
        reads.append(read)
    values = summed(3 * kw, vw) * row_scale
    gates = summed(3 * kw + vw, vw) * row_scale
    silu = gates * jax.nn.sigmoid(gates)
    for h in range(heads):
        at, to = slice(h * keys, (h + 1) * keys), slice(h * vals, (h + 1) * vals)
        read = reads[h] + jnp.sum(queries[:, at] * new_keys[:, at], axis=1, keepdims=True) * values[:, to]
        read = read * lax.rsqrt(jnp.mean(read * read, axis=1, keepdims=True) + epsilon) * gain_ref[...]
        gated_ref[:, to] = (read * silu[:, to]).astype(bf16)
    values_ref[...] = values
    factors_ref[0] = retain
    factors_ref[1] = new_keys


def readout(parts, state, narrowed, decay_offset, head_gain, depth):
    seqs, heads, keys, vals = state.shape
    outs = [
        jax.ShapeDtypeStruct((seqs, heads * vals), bf16),
        jax.ShapeDtypeStruct((2, seqs, heads * keys), f32),
        jax.ShapeDtypeStruct((seqs, heads * vals), f32),
    ]
    return pl.pallas_call(
        functools.partial(readout_kernel, len(parts), depth),
        out_shape=outs,
        in_specs=[VMEM] * (len(parts) + 3),
        out_specs=[VMEM] * 3,
        compiler_params=pltpu.CompilerParams(vmem_limit_bytes=8 * 2**20),
        cost_estimate=HEAVY,
        name="readout",
    )(*parts, narrowed, decay_offset.reshape(1, -1), head_gain.reshape(1, -1))


def update_kernel(first, count, factors_ref, values_ref, state_ref, *refs):
    out_hbm, tiles, sems = refs[-3:]
    seqs, heads, keys, vals = state_ref.shape
    rows = [factors_ref[n] for n in (0, 1)]
    if 2 * seqs % 8:
        rows.append(jnp.zeros((-2 * seqs % 8, heads * keys), f32))
    columns = jnp.concatenate(rows, axis=0).T
    copies = []
    for n in range(count):
        b = first + n
        for h in range(heads):
            at = slice(h * keys, (h + 1) * keys)
            keep, key = columns[at, b: b + 1], columns[at, seqs + b: seqs + b + 1]
            value = values_ref[b: b + 1, h * vals: (h + 1) * vals]
            tiles[n, h] = keep * state_ref[b, h] + key * value
            copies.append(pltpu.make_async_copy(tiles.at[n, h], out_hbm.at[b, h], sems.at[n, h]))
            copies[-1].start()
    for copy in copies:
        copy.wait()


def update(factors, values, state, first, count, *written):
    return pl.pallas_call(
        functools.partial(update_kernel, first, count),
        out_shape=jax.ShapeDtypeStruct(state.shape, f32),
        in_specs=[VMEM, VMEM, VMEM] + [pl.BlockSpec(memory_space=pl.ANY)] * len(written),
        out_specs=pl.BlockSpec(memory_space=pl.ANY),
        scratch_shapes=[pltpu.VMEM((count, *state.shape[1:]), f32), pltpu.SemaphoreType.DMA((count, state.shape[1]))],
        input_output_aliases={3: 0} if written else {},
        compiler_params=pltpu.CompilerParams(vmem_limit_bytes=8 * 2**20),
        cost_estimate=LIGHT,
        name="update",
    )(factors, values, state, *written)


def own_branch_kernel(gated_ref, w_ref, out_ref):
    seqs, width = gated_ref.shape
    gated = gated_ref[...].astype(f32)
    if seqs % 8:
        gated = jnp.concatenate([gated, jnp.zeros((-seqs % 8, width), f32)], axis=0)
    out_ref[...] = jnp.dot(gated.astype(bf16), w_ref[...], preferred_element_type=f32)[:seqs]


def branch_kernel(own_ref, *refs):
    *parts, w_ref, keep_ref, send_ref, rows = refs
    me, _ = here()
    seqs = own_ref.shape[0]
    far = jnp.concatenate([part[...].astype(f32) for part in parts] + [jnp.zeros(parts[0].shape, f32)], axis=0)
    far = jnp.dot(far.astype(bf16), w_ref[...], preferred_element_type=f32)
    rows[me] = own_ref[...]
    for k in range(1, len(parts) + 1):
        rows[me ^ k] = far[(k - 1) * seqs: k * seqs]
    for d in range(len(parts) + 1):
        keep_ref[d * seqs: (d + 1) * seqs, :] = rows[d]
    send_ref[...] = keep_ref[...].astype(bf16)


def branch_of(parts, own_w, other_w):
    seqs, width = parts[0].shape[0], own_w.shape[1]
    rows = seqs * len(parts)
    own = small(own_branch_kernel, jax.ShapeDtypeStruct((seqs, width), f32), parts[0], own_w, cost=LIGHT)
    outs = [jax.ShapeDtypeStruct((rows, width), kind) for kind in (f32, bf16)]
    return pl.pallas_call(
        branch_kernel,
        out_shape=outs,
        in_specs=[VMEM] * (len(parts) + 1),
        out_specs=[VMEM] * 2,
        scratch_shapes=[pltpu.VMEM((len(parts), seqs, width), f32)],
        compiler_params=pltpu.CompilerParams(vmem_limit_bytes=4 * 2**20),
        cost_estimate=HEAVY,
        name="branch",
    )(own, *parts[1:], other_w)


def hidden_of(owner, part, gain_ref, up_ref):
    width = part.shape[1]
    stream = part[...].astype(f32)
    normed = (stream * gain_ref[:, pl.ds(aligned(owner, width), width)]).astype(bf16)
    product = jnp.dot(normed, up_ref[pl.ds(aligned(owner, width), width), :], preferred_element_type=f32)
    return jnp.sum(stream * stream, axis=1, keepdims=True), product


def first_mixer_kernel(steps, *refs):
    *parts, gain_ref, up_ref, _, squares_ref, hidden_ref = refs
    me, _ = here()
    squares, hidden = 0.0, 0.0
    for k, part in zip(steps, parts):
        square, product = hidden_of(me ^ k, part, gain_ref, up_ref)
        squares += square
        hidden += product
    squares_ref[...] = jnp.broadcast_to(squares, squares_ref.shape)
    hidden_ref[...] = hidden


def mixer_kernel(steps, squares_ref, hidden_ref, *refs):
    *parts, gain_ref, up_ref, down_ref, keep_ref, give_ref, total = refs
    me, core = here()
    width = parts[0].shape[1]
    own = width // 2
    squares, hidden = squares_ref[:, :1], hidden_ref[...]
    for k, part in zip(steps, parts):
        square, product = hidden_of(me ^ k, part, gain_ref, up_ref)
        squares += square
        hidden += product
    hidden = hidden * lax.rsqrt(squares / up_ref.shape[0] + epsilon)
    squared = jnp.square(jnp.maximum(hidden, 0.0)).astype(bf16)
    total[...] = jnp.dot(squared, down_ref[...], preferred_element_type=f32)
    for k in range(keep_ref.shape[0]):
        side = core if k == 0 else 1 - core
        keep_ref[k] = total[:, pl.ds(aligned(2 * (me ^ k) + side, own), own)]
        give_ref[k] = total[:, pl.ds(aligned(2 * (me ^ k) + 1 - side, own), own)].astype(bf16)


def mixer(parts, mlp_gain, w_up, w_down):
    count = len(parts)
    rows, width = parts[0].shape
    early = (0, count - 1)
    late = tuple(range(1, count - 1))
    gain = mlp_gain.reshape(1, -1)
    params = dict(
        compiler_params=pltpu.CompilerParams(vmem_limit_bytes=6 * 2**20),
        cost_estimate=LIGHT,
    )
    begun = pl.pallas_call(
        functools.partial(first_mixer_kernel, early),
        out_shape=[jax.ShapeDtypeStruct((rows, 128), f32), jax.ShapeDtypeStruct((rows, w_up.shape[1]), f32)],
        in_specs=[VMEM] * 5,
        out_specs=[VMEM] * 2,
        name="first_mixer",
        **params,
    )(*[parts[k] for k in early], gain, w_up, w_down)
    outs = [jax.ShapeDtypeStruct((count, rows, width // 2), kind) for kind in (f32, bf16)]
    return pl.pallas_call(
        functools.partial(mixer_kernel, late),
        out_shape=outs,
        in_specs=[VMEM] * (5 + len(late)),
        out_specs=[VMEM] * 2,
        scratch_shapes=[pltpu.VMEM((rows, w_down.shape[1]), f32)],
        name="mixer",
        **params,
    )(*begun, *[parts[k] for k in late], gain, w_up, w_down)


def stream_kernel(branch_ref, came_ref, own_ref, other_ref, stream_ref):
    _, core = here()
    half = own_ref.shape[1]
    for ref, side in ((own_ref, core), (other_ref, 1 - core)):
        at = pl.ds(aligned(side, half), half)
        total = branch_ref[:, at] + came_ref[:, at].astype(f32)
        stream_ref[:, at] = (ref[...].astype(f32) + total).astype(bf16)


def pair_kernel(keep_ref, came_ref, *outs):
    for k, out in zip(range(len(outs) - 1, -1, -1), outs):
        out[...] = (keep_ref[k] + came_ref[k].astype(f32)).astype(out.dtype)


def last_kernel(stream_ref, *refs):
    *parts, out_ref = refs
    _, core = here()
    half = out_ref.shape[1]
    total = sum(p[...].astype(f32) for p in parts)
    out_ref[...] = (stream_ref[:, pl.ds(aligned(core, half), half)].astype(f32) + total).astype(bf16)


def small(body, outs, *args, cost=HEAVY):
    return pl.pallas_call(
        body,
        out_shape=outs,
        in_specs=[VMEM] * len(args),
        out_specs=jax.tree.map(lambda _: VMEM, outs),
        compiler_params=pltpu.CompilerParams(vmem_limit_bytes=2 * 2**20),
        cost_estimate=cost,
    )(*args)


def fused_steps(kv_size, tokens, state, mix_gain, weights, decay_offset, head_gain, w_out, mlp_gain, w_up, w_down):
    rows, half = tokens.shape
    depth = 2 * half * kv_size
    like = jax.ShapeDtypeStruct
    other = swap_cores(tokens)
    squares = small(clear_kernel, like((rows, 128), f32))
    parts = spread(project(squares, tokens, other, mix_gain, weights, kv_size), kv_size, 0)
    narrowed = narrow(state)
    gated, factors, values = readout(parts, state, narrowed, decay_offset, head_gain, depth)
    arrived = spread([gated] * kv_size, kv_size, 1)
    new_state = update(factors, values, state, 0, 1)
    new_state = update(factors, values, state, 1, 1, new_state)
    new_state = update(factors, values, state, 2, 2, new_state)
    w_other = swap_cores(w_out)
    branch, branch_sent = branch_of(arrived, w_out, w_other)
    stream = small(stream_kernel, like((rows, 2 * half), bf16), branch, swap_cores(branch_sent), tokens, other)
    keep, give = mixer(spread([stream] * kv_size, kv_size, 1), mlp_gain, w_up, w_down)
    outs = [like((rows, half), f32 if k == 0 else bf16) for k in range(kv_size - 1, -1, -1)]
    pieces = spread(small(pair_kernel, outs, keep, swap_cores(give))[::-1], kv_size, 1)
    return small(last_kernel, like((rows, half), bf16), stream, *pieces), new_state


def plain_steps(kv_size, tokens, state, mix_gain, weights, decay_offset, head_gain, w_out, mlp_gain, w_up, w_down):
    seqs, heads, keys, vals = state.shape
    rows, half = tokens.shape
    depth = 2 * half * kv_size
    core = lax.axis_index("tp")

    def exchange(blocks):
        return lax.all_to_all(blocks, "kv", 0, 0, tiled=True)

    def pick(pair):
        return jnp.where(core == 0, pair[0], pair[1]), jnp.where(core == 0, pair[1], pair[0])

    other = swap_cores(tokens)
    tok = jnp.concatenate(pick((tokens, other)), axis=1).astype(f32)
    squares = jnp.sum(tok * tok, axis=1, keepdims=True)
    scaled = (tok * mix_gain).astype(bf16)
    high = squares.astype(bf16).astype(f32)
    total = jnp.concatenate([jnp.dot(scaled, w, preferred_element_type=f32) for w in weights]
                            + [jnp.broadcast_to(x, (rows, 128)) for x in (high, squares - high)], axis=1)
    came = exchange(total.astype(bf16).reshape(kv_size, seqs, -1))
    total = jnp.sum(came.astype(f32), axis=0)
    kw, vw = heads * keys, heads * vals
    sums = total[:, 3 * kw + 2 * vw] + total[:, 3 * kw + 2 * vw + 128]
    total = total * lax.rsqrt(sums / depth + epsilon)[:, None]
    queries = (total[:, :kw] * keys ** (-0.5)).reshape(seqs, heads, keys)
    new_keys = total[:, kw: 2 * kw].reshape(seqs, heads, keys)
    retain = jax.nn.sigmoid(total[:, 2 * kw: 3 * kw] + decay_offset).reshape(seqs, heads, keys)
    values = total[:, 3 * kw: 3 * kw + vw].reshape(seqs, heads, vals)
    gates = total[:, 3 * kw + vw: 3 * kw + 2 * vw]
    new_state = retain[..., None] * state + new_keys[..., None] * values[:, :, None, :]
    read = jnp.einsum("bhk,bhkv->bhv", queries, new_state, precision=lax.Precision.HIGHEST)
    read = read * lax.rsqrt(jnp.mean(read * read, axis=2, keepdims=True) + epsilon) * head_gain
    gated = (read.reshape(seqs, vw) * jax.nn.silu(gates)).astype(bf16)
    gated = lax.all_gather(gated, "kv", axis=0, tiled=True)
    branch = jnp.dot(gated, w_out, preferred_element_type=f32)
    branch = branch + swap_cores(branch.astype(bf16)).astype(f32)
    stream_cols = (tok + branch).astype(bf16)
    stream = lax.all_gather(stream_cols, "kv", axis=1, tiled=True).astype(f32)
    scale = lax.rsqrt(jnp.mean(stream * stream, axis=1, keepdims=True) + epsilon)
    normed = (stream * mlp_gain).astype(bf16)
    hidden = jnp.dot(normed, w_up, preferred_element_type=f32) * scale
    squared = jnp.square(jax.nn.relu(hidden)).astype(bf16)
    down = jnp.dot(squared, w_down, preferred_element_type=f32)
    keep, give = pick(down.reshape(rows, kv_size, 2, half).transpose(2, 1, 0, 3))
    pair = keep + swap_cores(give.astype(bf16)).astype(f32)
    down_own = jnp.sum(exchange(pair.astype(bf16)).astype(f32), axis=0)
    stream_own, _ = pick((stream_cols[:, :half], stream_cols[:, half:]))
    return (stream_own.astype(f32) + down_own).astype(bf16), new_state


def shards(kv_size, tokens, state, mix_gain, w_query, w_key, w_decay, w_value, w_gate, *rest):
    steps = fused_steps if tokens.shape[1] % 128 == 0 and kv_size in (4, 8) else plain_steps
    return steps(kv_size, tokens, state, mix_gain, (w_query, w_key, w_decay, w_value, w_gate), *rest)


def solution(mesh):
    kv_size = mesh.shape["kv"]
    in_specs = (
        P("dp", ("kv", "tp")),
        P(("dp", "kv"), "tp", None, None),
        P("kv"),
        P("kv", "tp"),
        P("kv", "tp"),
        P("kv", "tp"),
        P("kv", "tp"),
        P("kv", "tp"),
        P("tp"),
        P(),
        P("tp", "kv"),
        P(),
        P(None, ("kv", "tp")),
        P(("kv", "tp"), None),
    )
    out_specs = (P("dp", ("kv", "tp")), P(("dp", "kv"), "tp", None, None))

    def body(*args):
        return shards(kv_size, *args)

    return jax.shard_map(body, mesh=mesh, in_specs=in_specs, out_specs=out_specs, check_vma=False)
```

```python
import functools

import jax
import jax.numpy as jnp
from jax import lax
from jax.experimental import pallas as pl
from jax.experimental.pallas import tpu as pltpu
from jax.sharding import PartitionSpec as P


epsilon = 1e-06
bf16, f32 = jnp.bfloat16, jnp.float32
VMEM = pl.BlockSpec(memory_space=pltpu.VMEM)
HEAVY = pl.CostEstimate(flops=2 * 10**10, bytes_accessed=2**20, transcendentals=0)
LIGHT = pl.CostEstimate(flops=2**17, bytes_accessed=2**17, transcendentals=0)


def swap_cores(value):
    return lax.ppermute(value, "tp", [(0, 1), (1, 0)])


def spread(pieces, kv_size, cross):
    came = []
    for k in range(1, kv_size):
        pairs = [(2 * i + c, 2 * (i ^ k) + (c ^ cross)) for i in range(kv_size) for c in (0, 1)]
        came.append(lax.ppermute(pieces[k], ("kv", "tp"), pairs))
    return [pieces[0]] + came


def here():
    return lax.axis_index("kv"), lax.axis_index("tp")


def aligned(start, step):
    return pl.multiple_of(start * step, step)


def clear_kernel(squares_ref):
    squares_ref[...] = jnp.zeros_like(squares_ref)


def put_blocks(total_ref, start, block):
    seqs = total_ref.shape[1]
    for d in range(total_ref.shape[0]):
        total_ref[d, :, start: start + block.shape[1]] = block[d * seqs: (d + 1) * seqs]


def project_parts(own, other, gain_ref, weights):
    _, core = here()
    half = own.shape[1]
    scaled = [
        ((x * gain_ref[:, pl.ds(aligned(side, half), half)]).astype(bf16), pl.ds(aligned(side, half), half))
        for x, side in ((own, core), (other, 1 - core))
    ]
    return [sum(jnp.dot(x, w[rows, :], preferred_element_type=f32) for x, rows in scaled) for w in weights]


def early_kernel(squares_ref, own_ref, other_ref, gain_ref, *refs):
    *weights, total = refs
    start = 0
    for block in project_parts(own_ref[...].astype(f32), other_ref[...].astype(f32), gain_ref, weights):
        put_blocks(total, start, block)
        start += block.shape[1]


def late_kernel(count, squares_ref, own_ref, other_ref, gain_ref, early_ref, *refs):
    weights, outs, total = refs[:-count - 1], refs[-count - 1: -1], refs[-1]
    me, _ = here()
    own, other = own_ref[...].astype(f32), other_ref[...].astype(f32)
    squares = squares_ref[...] + (
        jnp.sum(own * own, axis=1, keepdims=True) + jnp.sum(other * other, axis=1, keepdims=True))
    high = squares.astype(bf16).astype(f32)
    start = 0
    for block in project_parts(own, other, gain_ref, weights) + [high, squares - high]:
        put_blocks(total, start, block)
        start += block.shape[1]
    width = early_ref.shape[2]
    for k, out in zip(range(count - 1, -1, -1), outs):
        out[:, :width] = early_ref[me ^ k].astype(out.dtype)
        out[:, width:] = total[me ^ k].astype(out.dtype)


def project(squares, tokens, other, mix_gain, early, late, kv_size):
    seqs = other.shape[0] // kv_size
    params = dict(
        compiler_params=pltpu.CompilerParams(vmem_limit_bytes=6 * 2**20),
    )
    gain = mix_gain.reshape(1, -1)
    width, rest = sum(w.shape[1] for w in early), sum(w.shape[1] for w in late) + 256
    first = pl.pallas_call(
        early_kernel,
        out_shape=jax.ShapeDtypeStruct((kv_size, seqs, width), f32),
        in_specs=[VMEM] * (4 + len(early)),
        out_specs=VMEM,
        cost_estimate=LIGHT,
        name="early",
        **params,
    )(squares, tokens, other, gain, *early)
    outs = [jax.ShapeDtypeStruct((seqs, width + rest), f32 if k == 0 else bf16) for k in range(kv_size - 1, -1, -1)]
    return pl.pallas_call(
        functools.partial(late_kernel, kv_size),
        out_shape=outs,
        in_specs=[VMEM] * (5 + len(late)),
        out_specs=[VMEM] * kv_size,
        scratch_shapes=[pltpu.VMEM((kv_size, seqs, rest), f32)],
        cost_estimate=HEAVY,
        name="late",
        **params,
    )(squares, tokens, other, gain, first, *late)[::-1]


def narrow_kernel(state_ref, out_ref):
    out_ref[...] = state_ref[...].astype(bf16)


def narrow(state):
    return pl.pallas_call(
        narrow_kernel,
        out_shape=jax.ShapeDtypeStruct(state.shape, bf16),
        in_specs=[VMEM],
        out_specs=VMEM,
        compiler_params=pltpu.CompilerParams(vmem_limit_bytes=8 * 2**20),
        cost_estimate=LIGHT,
        name="narrow",
    )(state)


def readout_kernel(kv_size, depth, *refs):
    parts = refs[:kv_size]
    state_ref, offset_ref, gain_ref, gated_ref, factors_ref, values_ref = refs[kv_size:]
    seqs, heads, keys, vals = state_ref.shape
    kw, vw = heads * keys, heads * vals

    def summed(start, width):
        return sum(p[:, start: start + width].astype(f32) for p in parts)

    base = 3 * kw + 2 * vw
    sums = summed(base, 128)[:, :1] + summed(base + 128, 128)[:, :1]
    row_scale = lax.rsqrt(sums / depth + epsilon)
    queries = summed(2 * vw, kw) * row_scale * keys ** (-0.5)
    new_keys = summed(2 * vw + kw, kw) * row_scale
    retain = jax.nn.sigmoid(summed(2 * vw + 2 * kw, kw) * row_scale + offset_ref[...])
    kept = (queries * retain).astype(bf16)
    row = lax.broadcasted_iota(jnp.int32, (seqs, 1), 0)
    reads = []
    for h in range(heads):
        at = slice(h * keys, (h + 1) * keys)
        read = 0.0
        for b in range(seqs):
            product = jnp.dot(kept[:, at], state_ref[b, h], preferred_element_type=f32)
            read += jnp.where(row == b, product, 0.0)
        reads.append(read)
    values = summed(0, vw) * row_scale
    gates = summed(vw, vw) * row_scale
    silu = gates * jax.nn.sigmoid(gates)
    for h in range(heads):
        at, to = slice(h * keys, (h + 1) * keys), slice(h * vals, (h + 1) * vals)
        read = reads[h] + jnp.sum(queries[:, at] * new_keys[:, at], axis=1, keepdims=True) * values[:, to]
        read = read * lax.rsqrt(jnp.mean(read * read, axis=1, keepdims=True) + epsilon) * gain_ref[...]
        gated_ref[:, to] = (read * silu[:, to]).astype(bf16)
    values_ref[...] = values
    factors_ref[0] = retain
    factors_ref[1] = new_keys


def readout(parts, state, narrowed, decay_offset, head_gain, depth):
    seqs, heads, keys, vals = state.shape
    outs = [
        jax.ShapeDtypeStruct((seqs, heads * vals), bf16),
        jax.ShapeDtypeStruct((2, seqs, heads * keys), f32),
        jax.ShapeDtypeStruct((seqs, heads * vals), f32),
    ]
    return pl.pallas_call(
        functools.partial(readout_kernel, len(parts), depth),
        out_shape=outs,
        in_specs=[VMEM] * (len(parts) + 3),
        out_specs=[VMEM] * 3,
        compiler_params=pltpu.CompilerParams(vmem_limit_bytes=8 * 2**20),
        cost_estimate=HEAVY,
        name="readout",
    )(*parts, narrowed, decay_offset.reshape(1, -1), head_gain.reshape(1, -1))


def update_kernel(first, count, factors_ref, values_ref, state_ref, *refs):
    out_hbm, tiles, sems = refs[-3:]
    seqs, heads, keys, vals = state_ref.shape
    rows = [factors_ref[n] for n in (0, 1)]
    if 2 * seqs % 8:
        rows.append(jnp.zeros((-2 * seqs % 8, heads * keys), f32))
    columns = jnp.concatenate(rows, axis=0).T
    copies = []
    for n in range(count):
        b = first + n
        for h in range(heads):
            at = slice(h * keys, (h + 1) * keys)
            keep, key = columns[at, b: b + 1], columns[at, seqs + b: seqs + b + 1]
            value = values_ref[b: b + 1, h * vals: (h + 1) * vals]
            tiles[n, h] = keep * state_ref[b, h] + key * value
            copies.append(pltpu.make_async_copy(tiles.at[n, h], out_hbm.at[b, h], sems.at[n, h]))
            copies[-1].start()
    for copy in copies:
        copy.wait()


def update(factors, values, state, first, count, *written):
    return pl.pallas_call(
        functools.partial(update_kernel, first, count),
        out_shape=jax.ShapeDtypeStruct(state.shape, f32),
        in_specs=[VMEM, VMEM, VMEM] + [pl.BlockSpec(memory_space=pl.ANY)] * len(written),
        out_specs=pl.BlockSpec(memory_space=pl.ANY),
        scratch_shapes=[pltpu.VMEM((count, *state.shape[1:]), f32), pltpu.SemaphoreType.DMA((count, state.shape[1]))],
        input_output_aliases={3: 0} if written else {},
        compiler_params=pltpu.CompilerParams(vmem_limit_bytes=8 * 2**20),
        cost_estimate=LIGHT,
        name="update",
    )(factors, values, state, *written)


def own_branch_kernel(gated_ref, w_ref, out_ref):
    seqs, width = gated_ref.shape
    gated = gated_ref[...].astype(f32)
    if seqs % 8:
        gated = jnp.concatenate([gated, jnp.zeros((-seqs % 8, width), f32)], axis=0)
    out_ref[...] = jnp.dot(gated.astype(bf16), w_ref[...], preferred_element_type=f32)[:seqs]


def branch_kernel(own_ref, *refs):
    *parts, w_ref, keep_ref, send_ref, rows = refs
    me, _ = here()
    seqs = own_ref.shape[0]
    far = jnp.concatenate([part[...].astype(f32) for part in parts] + [jnp.zeros(parts[0].shape, f32)], axis=0)
    far = jnp.dot(far.astype(bf16), w_ref[...], preferred_element_type=f32)
    rows[me] = own_ref[...]
    for k in range(1, len(parts) + 1):
        rows[me ^ k] = far[(k - 1) * seqs: k * seqs]
    for d in range(len(parts) + 1):
        keep_ref[d * seqs: (d + 1) * seqs, :] = rows[d]
    send_ref[...] = keep_ref[...].astype(bf16)


def branch_of(parts, own_w, other_w):
    seqs, width = parts[0].shape[0], own_w.shape[1]
    rows = seqs * len(parts)
    own = small(own_branch_kernel, jax.ShapeDtypeStruct((seqs, width), f32), parts[0], own_w, cost=LIGHT)
    outs = [jax.ShapeDtypeStruct((rows, width), kind) for kind in (f32, bf16)]
    return pl.pallas_call(
        branch_kernel,
        out_shape=outs,
        in_specs=[VMEM] * (len(parts) + 1),
        out_specs=[VMEM] * 2,
        scratch_shapes=[pltpu.VMEM((len(parts), seqs, width), f32)],
        compiler_params=pltpu.CompilerParams(vmem_limit_bytes=4 * 2**20),
        cost_estimate=HEAVY,
        name="branch",
    )(own, *parts[1:], other_w)


def hidden_of(owner, part, gain_ref, up_ref):
    width = part.shape[1]
    stream = part[...].astype(f32)
    normed = (stream * gain_ref[:, pl.ds(aligned(owner, width), width)]).astype(bf16)
    product = jnp.dot(normed, up_ref[pl.ds(aligned(owner, width), width), :], preferred_element_type=f32)
    return jnp.sum(stream * stream, axis=1, keepdims=True), product


def first_mixer_kernel(steps, *refs):
    *parts, gain_ref, up_ref, _, squares_ref, hidden_ref = refs
    me, _ = here()
    squares, hidden = 0.0, 0.0
    for k, part in zip(steps, parts):
        square, product = hidden_of(me ^ k, part, gain_ref, up_ref)
        squares += square
        hidden += product
    squares_ref[...] = jnp.broadcast_to(squares, squares_ref.shape)
    hidden_ref[...] = hidden


def mixer_kernel(steps, squares_ref, hidden_ref, *refs):
    *parts, gain_ref, up_ref, down_ref, keep_ref, give_ref, total = refs
    me, core = here()
    width = parts[0].shape[1]
    own = width // 2
    squares, hidden = squares_ref[:, :1], hidden_ref[...]
    for k, part in zip(steps, parts):
        square, product = hidden_of(me ^ k, part, gain_ref, up_ref)
        squares += square
        hidden += product
    hidden = hidden * lax.rsqrt(squares / up_ref.shape[0] + epsilon)
    squared = jnp.square(jnp.maximum(hidden, 0.0)).astype(bf16)
    total[...] = jnp.dot(squared, down_ref[...], preferred_element_type=f32)
    for k in range(keep_ref.shape[0]):
        side = core if k == 0 else 1 - core
        keep_ref[k] = total[:, pl.ds(aligned(2 * (me ^ k) + side, own), own)]
        give_ref[k] = total[:, pl.ds(aligned(2 * (me ^ k) + 1 - side, own), own)].astype(bf16)


def mixer(parts, mlp_gain, w_up, w_down):
    count = len(parts)
    rows, width = parts[0].shape
    early = (0, count - 1)
    late = tuple(range(1, count - 1))
    gain = mlp_gain.reshape(1, -1)
    params = dict(
        compiler_params=pltpu.CompilerParams(vmem_limit_bytes=6 * 2**20),
        cost_estimate=LIGHT,
    )
    begun = pl.pallas_call(
        functools.partial(first_mixer_kernel, early),
        out_shape=[jax.ShapeDtypeStruct((rows, 128), f32), jax.ShapeDtypeStruct((rows, w_up.shape[1]), f32)],
        in_specs=[VMEM] * 5,
        out_specs=[VMEM] * 2,
        name="first_mixer",
        **params,
    )(*[parts[k] for k in early], gain, w_up, w_down)
    outs = [jax.ShapeDtypeStruct((count, rows, width // 2), kind) for kind in (f32, bf16)]
    return pl.pallas_call(
        functools.partial(mixer_kernel, late),
        out_shape=outs,
        in_specs=[VMEM] * (5 + len(late)),
        out_specs=[VMEM] * 2,
        scratch_shapes=[pltpu.VMEM((rows, w_down.shape[1]), f32)],
        name="mixer",
        **params,
    )(*begun, *[parts[k] for k in late], gain, w_up, w_down)


def stream_kernel(branch_ref, came_ref, own_ref, other_ref, stream_ref):
    _, core = here()
    half = own_ref.shape[1]
    for ref, side in ((own_ref, core), (other_ref, 1 - core)):
        at = pl.ds(aligned(side, half), half)
        total = branch_ref[:, at] + came_ref[:, at].astype(f32)
        stream_ref[:, at] = (ref[...].astype(f32) + total).astype(bf16)


def pair_kernel(keep_ref, came_ref, *outs):
    for k, out in zip(range(len(outs) - 1, -1, -1), outs):
        out[...] = (keep_ref[k] + came_ref[k].astype(f32)).astype(out.dtype)


def last_kernel(stream_ref, *refs):
    *parts, out_ref = refs
    _, core = here()
    half = out_ref.shape[1]
    total = sum(p[...].astype(f32) for p in parts)
    out_ref[...] = (stream_ref[:, pl.ds(aligned(core, half), half)].astype(f32) + total).astype(bf16)


def small(body, outs, *args, cost=HEAVY):
    return pl.pallas_call(
        body,
        out_shape=outs,
        in_specs=[VMEM] * len(args),
        out_specs=jax.tree.map(lambda _: VMEM, outs),
        compiler_params=pltpu.CompilerParams(vmem_limit_bytes=2 * 2**20),
        cost_estimate=cost,
    )(*args)


def fused_steps(kv_size, tokens, state, mix_gain, weights, decay_offset, head_gain, w_out, mlp_gain, w_up, w_down):
    rows, half = tokens.shape
    depth = 2 * half * kv_size
    like = jax.ShapeDtypeStruct
    other = swap_cores(tokens)
    squares = small(clear_kernel, like((rows, 128), f32))
    parts = spread(project(squares, tokens, other, mix_gain, weights[3:], weights[:3], kv_size), kv_size, 0)
    narrowed = narrow(state)
    gated, factors, values = readout(parts, state, narrowed, decay_offset, head_gain, depth)
    arrived = spread([gated] * kv_size, kv_size, 1)
    new_state = update(factors, values, state, 0, 1)
    new_state = update(factors, values, state, 1, 1, new_state)
    new_state = update(factors, values, state, 2, 2, new_state)
    w_other = swap_cores(w_out)
    branch, branch_sent = branch_of(arrived, w_out, w_other)
    stream = small(stream_kernel, like((rows, 2 * half), bf16), branch, swap_cores(branch_sent), tokens, other)
    keep, give = mixer(spread([stream] * kv_size, kv_size, 1), mlp_gain, w_up, w_down)
    outs = [like((rows, half), f32 if k == 0 else bf16) for k in range(kv_size - 1, -1, -1)]
    pieces = spread(small(pair_kernel, outs, keep, swap_cores(give))[::-1], kv_size, 1)
    return small(last_kernel, like((rows, half), bf16), stream, *pieces), new_state


def plain_steps(kv_size, tokens, state, mix_gain, weights, decay_offset, head_gain, w_out, mlp_gain, w_up, w_down):
    seqs, heads, keys, vals = state.shape
    rows, half = tokens.shape
    depth = 2 * half * kv_size
    core = lax.axis_index("tp")

    def exchange(blocks):
        return lax.all_to_all(blocks, "kv", 0, 0, tiled=True)

    def pick(pair):
        return jnp.where(core == 0, pair[0], pair[1]), jnp.where(core == 0, pair[1], pair[0])

    other = swap_cores(tokens)
    tok = jnp.concatenate(pick((tokens, other)), axis=1).astype(f32)
    squares = jnp.sum(tok * tok, axis=1, keepdims=True)
    scaled = (tok * mix_gain).astype(bf16)
    high = squares.astype(bf16).astype(f32)
    total = jnp.concatenate([jnp.dot(scaled, w, preferred_element_type=f32) for w in weights]
                            + [jnp.broadcast_to(x, (rows, 128)) for x in (high, squares - high)], axis=1)
    came = exchange(total.astype(bf16).reshape(kv_size, seqs, -1))
    total = jnp.sum(came.astype(f32), axis=0)
    kw, vw = heads * keys, heads * vals
    sums = total[:, 3 * kw + 2 * vw] + total[:, 3 * kw + 2 * vw + 128]
    total = total * lax.rsqrt(sums / depth + epsilon)[:, None]
    queries = (total[:, :kw] * keys ** (-0.5)).reshape(seqs, heads, keys)
    new_keys = total[:, kw: 2 * kw].reshape(seqs, heads, keys)
    retain = jax.nn.sigmoid(total[:, 2 * kw: 3 * kw] + decay_offset).reshape(seqs, heads, keys)
    values = total[:, 3 * kw: 3 * kw + vw].reshape(seqs, heads, vals)
    gates = total[:, 3 * kw + vw: 3 * kw + 2 * vw]
    new_state = retain[..., None] * state + new_keys[..., None] * values[:, :, None, :]
    read = jnp.einsum("bhk,bhkv->bhv", queries, new_state, precision=lax.Precision.HIGHEST)
    read = read * lax.rsqrt(jnp.mean(read * read, axis=2, keepdims=True) + epsilon) * head_gain
    gated = (read.reshape(seqs, vw) * jax.nn.silu(gates)).astype(bf16)
    gated = lax.all_gather(gated, "kv", axis=0, tiled=True)
    branch = jnp.dot(gated, w_out, preferred_element_type=f32)
    branch = branch + swap_cores(branch.astype(bf16)).astype(f32)
    stream_cols = (tok + branch).astype(bf16)
    stream = lax.all_gather(stream_cols, "kv", axis=1, tiled=True).astype(f32)
    scale = lax.rsqrt(jnp.mean(stream * stream, axis=1, keepdims=True) + epsilon)
    normed = (stream * mlp_gain).astype(bf16)
    hidden = jnp.dot(normed, w_up, preferred_element_type=f32) * scale
    squared = jnp.square(jax.nn.relu(hidden)).astype(bf16)
    down = jnp.dot(squared, w_down, preferred_element_type=f32)
    keep, give = pick(down.reshape(rows, kv_size, 2, half).transpose(2, 1, 0, 3))
    pair = keep + swap_cores(give.astype(bf16)).astype(f32)
    down_own = jnp.sum(exchange(pair.astype(bf16)).astype(f32), axis=0)
    stream_own, _ = pick((stream_cols[:, :half], stream_cols[:, half:]))
    return (stream_own.astype(f32) + down_own).astype(bf16), new_state


def shards(kv_size, tokens, state, mix_gain, w_query, w_key, w_decay, w_value, w_gate, *rest):
    steps = fused_steps if tokens.shape[1] % 128 == 0 and kv_size in (4, 8) else plain_steps
    return steps(kv_size, tokens, state, mix_gain, (w_query, w_key, w_decay, w_value, w_gate), *rest)


def solution(mesh):
    kv_size = mesh.shape["kv"]
    in_specs = (
        P("dp", ("kv", "tp")),
        P(("dp", "kv"), "tp", None, None),
        P("kv"),
        P("kv", "tp"),
        P("kv", "tp"),
        P("kv", "tp"),
        P("kv", "tp"),
        P("kv", "tp"),
        P("tp"),
        P(),
        P("tp", "kv"),
        P(),
        P(None, ("kv", "tp")),
        P(("kv", "tp"), None),
    )
    out_specs = (P("dp", ("kv", "tp")), P(("dp", "kv"), "tp", None, None))

    def body(*args):
        return shards(kv_size, *args)

    return jax.shard_map(body, mesh=mesh, in_specs=in_specs, out_specs=out_specs, check_vma=False)
```

```python
import functools

import jax
import jax.numpy as jnp
from jax import lax
from jax.experimental import pallas as pl
from jax.experimental.pallas import tpu as pltpu
from jax.sharding import PartitionSpec as P


epsilon = 1e-06
bf16, f32 = jnp.bfloat16, jnp.float32
VMEM = pl.BlockSpec(memory_space=pltpu.VMEM)
HEAVY = pl.CostEstimate(flops=2 * 10**10, bytes_accessed=2**20, transcendentals=0)
LIGHT = pl.CostEstimate(flops=2**17, bytes_accessed=2**17, transcendentals=0)


def swap_cores(value):
    return lax.ppermute(value, "tp", [(0, 1), (1, 0)])


def spread(pieces, kv_size, cross):
    came = []
    for k in range(1, kv_size):
        pairs = [(2 * i + c, 2 * (i ^ k) + (c ^ cross)) for i in range(kv_size) for c in (0, 1)]
        came.append(lax.ppermute(pieces[k], ("kv", "tp"), pairs))
    return [pieces[0]] + came


def here():
    return lax.axis_index("kv"), lax.axis_index("tp")


def aligned(start, step):
    return pl.multiple_of(start * step, step)


def clear_kernel(squares_ref):
    squares_ref[...] = jnp.zeros_like(squares_ref)


def put_blocks(total_ref, start, block):
    seqs = total_ref.shape[1]
    for d in range(total_ref.shape[0]):
        total_ref[d, :, start: start + block.shape[1]] = block[d * seqs: (d + 1) * seqs]


def project_parts(own, other, gain_ref, weights):
    _, core = here()
    half = own.shape[1]
    scaled = [
        ((x * gain_ref[:, pl.ds(aligned(side, half), half)]).astype(bf16), pl.ds(aligned(side, half), half))
        for x, side in ((own, core), (other, 1 - core))
    ]
    return [sum(jnp.dot(x, w[rows, :], preferred_element_type=f32) for x, rows in scaled) for w in weights]


def early_kernel(squares_ref, own_ref, other_ref, gain_ref, *refs):
    *weights, total = refs
    start = 0
    for block in project_parts(own_ref[...].astype(f32), other_ref[...].astype(f32), gain_ref, weights):
        put_blocks(total, start, block)
        start += block.shape[1]


def late_kernel(count, squares_ref, own_ref, other_ref, gain_ref, early_ref, *refs):
    weights, outs, total = refs[:-count - 1], refs[-count - 1: -1], refs[-1]
    me, _ = here()
    own, other = own_ref[...].astype(f32), other_ref[...].astype(f32)
    squares = squares_ref[...] + (
        jnp.sum(own * own, axis=1, keepdims=True) + jnp.sum(other * other, axis=1, keepdims=True))
    high = squares.astype(bf16).astype(f32)
    start = 0
    for block in project_parts(own, other, gain_ref, weights) + [high, squares - high]:
        put_blocks(total, start, block)
        start += block.shape[1]
    width = early_ref.shape[2]
    for k, out in zip(range(count - 1, -1, -1), outs):
        out[:, :width] = early_ref[me ^ k].astype(out.dtype)
        out[:, width:] = total[me ^ k].astype(out.dtype)


def project(squares, tokens, other, mix_gain, early, late, kv_size):
    seqs = other.shape[0] // kv_size
    params = dict(
        compiler_params=pltpu.CompilerParams(vmem_limit_bytes=6 * 2**20),
    )
    gain = mix_gain.reshape(1, -1)
    width, rest = sum(w.shape[1] for w in early), sum(w.shape[1] for w in late) + 256
    first = pl.pallas_call(
        early_kernel,
        out_shape=jax.ShapeDtypeStruct((kv_size, seqs, width), f32),
        in_specs=[VMEM] * (4 + len(early)),
        out_specs=VMEM,
        cost_estimate=LIGHT,
        name="early",
        **params,
    )(squares, tokens, other, gain, *early)
    outs = [jax.ShapeDtypeStruct((seqs, width + rest), f32 if k == 0 else bf16) for k in range(kv_size - 1, -1, -1)]
    return pl.pallas_call(
        functools.partial(late_kernel, kv_size),
        out_shape=outs,
        in_specs=[VMEM] * (5 + len(late)),
        out_specs=[VMEM] * kv_size,
        scratch_shapes=[pltpu.VMEM((kv_size, seqs, rest), f32)],
        cost_estimate=HEAVY,
        name="late",
        **params,
    )(squares, tokens, other, gain, first, *late)[::-1]


def narrow_kernel(state_ref, out_ref):
    out_ref[...] = state_ref[...].astype(bf16)


def narrow(state):
    return pl.pallas_call(
        narrow_kernel,
        out_shape=jax.ShapeDtypeStruct(state.shape, bf16),
        in_specs=[VMEM],
        out_specs=VMEM,
        compiler_params=pltpu.CompilerParams(vmem_limit_bytes=8 * 2**20),
        cost_estimate=LIGHT,
        name="narrow",
    )(state)


def readout_kernel(kv_size, depth, *refs):
    parts = refs[:kv_size]
    state_ref, offset_ref, gain_ref, gated_ref, factors_ref, values_ref = refs[kv_size:]
    seqs, heads, keys, vals = state_ref.shape
    kw, vw = heads * keys, heads * vals

    def summed(start, width):
        return sum(p[:, start: start + width].astype(f32) for p in parts)

    base = 3 * kw + 2 * vw
    sums = summed(base, 128)[:, :1] + summed(base + 128, 128)[:, :1]
    row_scale = lax.rsqrt(sums / depth + epsilon)
    queries = summed(2 * vw, kw) * row_scale * keys ** (-0.5)
    new_keys = summed(2 * vw + kw, kw) * row_scale
    retain = jax.nn.sigmoid(summed(2 * vw + 2 * kw, kw) * row_scale + offset_ref[...])
    kept = (queries * retain).astype(bf16)
    row = lax.broadcasted_iota(jnp.int32, (seqs, 1), 0)
    reads = []
    for h in range(heads):
        at = slice(h * keys, (h + 1) * keys)
        read = 0.0
        for b in range(seqs):
            product = jnp.dot(kept[:, at], state_ref[b, h], preferred_element_type=f32)
            read += jnp.where(row == b, product, 0.0)
        reads.append(read)
    values = summed(0, vw) * row_scale
    gates = summed(vw, vw) * row_scale
    silu = gates * jax.nn.sigmoid(gates)
    for h in range(heads):
        at, to = slice(h * keys, (h + 1) * keys), slice(h * vals, (h + 1) * vals)
        read = reads[h] + jnp.sum(queries[:, at] * new_keys[:, at], axis=1, keepdims=True) * values[:, to]
        read = read * lax.rsqrt(jnp.mean(read * read, axis=1, keepdims=True) + epsilon) * gain_ref[...]
        gated_ref[:, to] = (read * silu[:, to]).astype(bf16)
    values_ref[...] = values
    factors_ref[0] = retain
    factors_ref[1] = new_keys


def readout(parts, state, narrowed, decay_offset, head_gain, depth):
    seqs, heads, keys, vals = state.shape
    outs = [
        jax.ShapeDtypeStruct((seqs, heads * vals), bf16),
        jax.ShapeDtypeStruct((2, seqs, heads * keys), f32),
        jax.ShapeDtypeStruct((seqs, heads * vals), f32),
    ]
    return pl.pallas_call(
        functools.partial(readout_kernel, len(parts), depth),
        out_shape=outs,
        in_specs=[VMEM] * (len(parts) + 3),
        out_specs=[VMEM] * 3,
        compiler_params=pltpu.CompilerParams(vmem_limit_bytes=8 * 2**20),
        cost_estimate=HEAVY,
        name="readout",
    )(*parts, narrowed, decay_offset.reshape(1, -1), head_gain.reshape(1, -1))


def update_kernel(first, count, factors_ref, values_ref, state_ref, *refs):
    out_hbm, tiles, sems = refs[-3:]
    seqs, heads, keys, vals = state_ref.shape
    rows = [factors_ref[n] for n in (0, 1)]
    if 2 * seqs % 8:
        rows.append(jnp.zeros((-2 * seqs % 8, heads * keys), f32))
    columns = jnp.concatenate(rows, axis=0).T
    copies = []
    for n in range(count):
        b, h = divmod(first + n, heads)
        at = slice(h * keys, (h + 1) * keys)
        keep, key = columns[at, b: b + 1], columns[at, seqs + b: seqs + b + 1]
        value = values_ref[b: b + 1, h * vals: (h + 1) * vals]
        tiles[n] = keep * state_ref[b, h] + key * value
        copies.append(pltpu.make_async_copy(tiles.at[n], out_hbm.at[b, h], sems.at[n]))
        copies[-1].start()
    for copy in copies:
        copy.wait()


def update(factors, values, state, first, count, *written):
    return pl.pallas_call(
        functools.partial(update_kernel, first, count),
        out_shape=jax.ShapeDtypeStruct(state.shape, f32),
        in_specs=[VMEM, VMEM, VMEM] + [pl.BlockSpec(memory_space=pl.ANY)] * len(written),
        out_specs=pl.BlockSpec(memory_space=pl.ANY),
        scratch_shapes=[pltpu.VMEM((count, *state.shape[2:]), f32), pltpu.SemaphoreType.DMA((count,))],
        input_output_aliases={3: 0} if written else {},
        compiler_params=pltpu.CompilerParams(vmem_limit_bytes=8 * 2**20),
        cost_estimate=LIGHT,
        name="update",
    )(factors, values, state, *written)


def own_branch_kernel(gated_ref, w_ref, out_ref):
    seqs, width = gated_ref.shape
    gated = gated_ref[...].astype(f32)
    if seqs % 8:
        gated = jnp.concatenate([gated, jnp.zeros((-seqs % 8, width), f32)], axis=0)
    out_ref[...] = jnp.dot(gated.astype(bf16), w_ref[...], preferred_element_type=f32)[:seqs]


def branch_kernel(own_ref, *refs):
    *parts, w_ref, keep_ref, send_ref, rows = refs
    me, _ = here()
    seqs = own_ref.shape[0]
    far = jnp.concatenate([part[...].astype(f32) for part in parts] + [jnp.zeros(parts[0].shape, f32)], axis=0)
    far = jnp.dot(far.astype(bf16), w_ref[...], preferred_element_type=f32)
    rows[me] = own_ref[...]
    for k in range(1, len(parts) + 1):
        rows[me ^ k] = far[(k - 1) * seqs: k * seqs]
    for d in range(len(parts) + 1):
        keep_ref[d * seqs: (d + 1) * seqs, :] = rows[d]
    send_ref[...] = keep_ref[...].astype(bf16)


def branch_of(parts, own_w, other_w):
    seqs, width = parts[0].shape[0], own_w.shape[1]
    rows = seqs * len(parts)
    own = small(own_branch_kernel, jax.ShapeDtypeStruct((seqs, width), f32), parts[0], own_w, cost=LIGHT)
    outs = [jax.ShapeDtypeStruct((rows, width), kind) for kind in (f32, bf16)]
    return pl.pallas_call(
        branch_kernel,
        out_shape=outs,
        in_specs=[VMEM] * (len(parts) + 1),
        out_specs=[VMEM] * 2,
        scratch_shapes=[pltpu.VMEM((len(parts), seqs, width), f32)],
        compiler_params=pltpu.CompilerParams(vmem_limit_bytes=4 * 2**20),
        cost_estimate=HEAVY,
        name="branch",
    )(own, *parts[1:], other_w)


def hidden_of(owner, part, gain_ref, up_ref):
    width = part.shape[1]
    stream = part[...].astype(f32)
    normed = (stream * gain_ref[:, pl.ds(aligned(owner, width), width)]).astype(bf16)
    product = jnp.dot(normed, up_ref[pl.ds(aligned(owner, width), width), :], preferred_element_type=f32)
    return jnp.sum(stream * stream, axis=1, keepdims=True), product


def first_mixer_kernel(steps, *refs):
    *parts, gain_ref, up_ref, _, squares_ref, hidden_ref = refs
    me, _ = here()
    squares, hidden = 0.0, 0.0
    for k, part in zip(steps, parts):
        square, product = hidden_of(me ^ k, part, gain_ref, up_ref)
        squares += square
        hidden += product
    squares_ref[...] = jnp.broadcast_to(squares, squares_ref.shape)
    hidden_ref[...] = hidden


def mixer_kernel(steps, squares_ref, hidden_ref, *refs):
    *parts, gain_ref, up_ref, down_ref, keep_ref, give_ref, total = refs
    me, core = here()
    width = parts[0].shape[1]
    own = width // 2
    squares, hidden = squares_ref[:, :1], hidden_ref[...]
    for k, part in zip(steps, parts):
        square, product = hidden_of(me ^ k, part, gain_ref, up_ref)
        squares += square
        hidden += product
    hidden = hidden * lax.rsqrt(squares / up_ref.shape[0] + epsilon)
    squared = jnp.square(jnp.maximum(hidden, 0.0)).astype(bf16)
    total[...] = jnp.dot(squared, down_ref[...], preferred_element_type=f32)
    for k in range(keep_ref.shape[0]):
        side = core if k == 0 else 1 - core
        keep_ref[k] = total[:, pl.ds(aligned(2 * (me ^ k) + side, own), own)]
        give_ref[k] = total[:, pl.ds(aligned(2 * (me ^ k) + 1 - side, own), own)].astype(bf16)


def mixer(parts, mlp_gain, w_up, w_down):
    count = len(parts)
    rows, width = parts[0].shape
    early = (0, count - 1)
    late = tuple(range(1, count - 1))
    gain = mlp_gain.reshape(1, -1)
    params = dict(
        compiler_params=pltpu.CompilerParams(vmem_limit_bytes=6 * 2**20),
        cost_estimate=LIGHT,
    )
    begun = pl.pallas_call(
        functools.partial(first_mixer_kernel, early),
        out_shape=[jax.ShapeDtypeStruct((rows, 128), f32), jax.ShapeDtypeStruct((rows, w_up.shape[1]), f32)],
        in_specs=[VMEM] * 5,
        out_specs=[VMEM] * 2,
        name="first_mixer",
        **params,
    )(*[parts[k] for k in early], gain, w_up, w_down)
    outs = [jax.ShapeDtypeStruct((count, rows, width // 2), kind) for kind in (f32, bf16)]
    return pl.pallas_call(
        functools.partial(mixer_kernel, late),
        out_shape=outs,
        in_specs=[VMEM] * (5 + len(late)),
        out_specs=[VMEM] * 2,
        scratch_shapes=[pltpu.VMEM((rows, w_down.shape[1]), f32)],
        name="mixer",
        **params,
    )(*begun, *[parts[k] for k in late], gain, w_up, w_down)


def stream_kernel(branch_ref, came_ref, own_ref, other_ref, stream_ref):
    _, core = here()
    half = own_ref.shape[1]
    for ref, side in ((own_ref, core), (other_ref, 1 - core)):
        at = pl.ds(aligned(side, half), half)
        total = branch_ref[:, at] + came_ref[:, at].astype(f32)
        stream_ref[:, at] = (ref[...].astype(f32) + total).astype(bf16)


def pair_kernel(keep_ref, came_ref, *outs):
    for k, out in zip(range(len(outs) - 1, -1, -1), outs):
        out[...] = (keep_ref[k] + came_ref[k].astype(f32)).astype(out.dtype)


def last_kernel(stream_ref, *refs):
    *parts, out_ref = refs
    _, core = here()
    half = out_ref.shape[1]
    total = sum(p[...].astype(f32) for p in parts)
    out_ref[...] = (stream_ref[:, pl.ds(aligned(core, half), half)].astype(f32) + total).astype(bf16)


def small(body, outs, *args, cost=HEAVY):
    return pl.pallas_call(
        body,
        out_shape=outs,
        in_specs=[VMEM] * len(args),
        out_specs=jax.tree.map(lambda _: VMEM, outs),
        compiler_params=pltpu.CompilerParams(vmem_limit_bytes=2 * 2**20),
        cost_estimate=cost,
    )(*args)


def fused_steps(kv_size, tokens, state, mix_gain, weights, decay_offset, head_gain, w_out, mlp_gain, w_up, w_down):
    rows, half = tokens.shape
    depth = 2 * half * kv_size
    like = jax.ShapeDtypeStruct
    other = swap_cores(tokens)
    squares = small(clear_kernel, like((rows, 128), f32))
    parts = spread(project(squares, tokens, other, mix_gain, weights[3:], weights[:3], kv_size), kv_size, 0)
    narrowed = narrow(state)
    gated, factors, values = readout(parts, state, narrowed, decay_offset, head_gain, depth)
    arrived = spread([gated] * kv_size, kv_size, 1)
    new_state = update(factors, values, state, 0, 1)
    new_state = update(factors, values, state, 1, 3, new_state)
    new_state = update(factors, values, state, 4, 4, new_state)
    w_other = swap_cores(w_out)
    branch, branch_sent = branch_of(arrived, w_out, w_other)
    stream = small(stream_kernel, like((rows, 2 * half), bf16), branch, swap_cores(branch_sent), tokens, other)
    keep, give = mixer(spread([stream] * kv_size, kv_size, 1), mlp_gain, w_up, w_down)
    outs = [like((rows, half), f32 if k == 0 else bf16) for k in range(kv_size - 1, -1, -1)]
    pieces = spread(small(pair_kernel, outs, keep, swap_cores(give))[::-1], kv_size, 1)
    return small(last_kernel, like((rows, half), bf16), stream, *pieces), new_state


def plain_steps(kv_size, tokens, state, mix_gain, weights, decay_offset, head_gain, w_out, mlp_gain, w_up, w_down):
    seqs, heads, keys, vals = state.shape
    rows, half = tokens.shape
    depth = 2 * half * kv_size
    core = lax.axis_index("tp")

    def exchange(blocks):
        return lax.all_to_all(blocks, "kv", 0, 0, tiled=True)

    def pick(pair):
        return jnp.where(core == 0, pair[0], pair[1]), jnp.where(core == 0, pair[1], pair[0])

    other = swap_cores(tokens)
    tok = jnp.concatenate(pick((tokens, other)), axis=1).astype(f32)
    squares = jnp.sum(tok * tok, axis=1, keepdims=True)
    scaled = (tok * mix_gain).astype(bf16)
    high = squares.astype(bf16).astype(f32)
    total = jnp.concatenate([jnp.dot(scaled, w, preferred_element_type=f32) for w in weights]
                            + [jnp.broadcast_to(x, (rows, 128)) for x in (high, squares - high)], axis=1)
    came = exchange(total.astype(bf16).reshape(kv_size, seqs, -1))
    total = jnp.sum(came.astype(f32), axis=0)
    kw, vw = heads * keys, heads * vals
    sums = total[:, 3 * kw + 2 * vw] + total[:, 3 * kw + 2 * vw + 128]
    total = total * lax.rsqrt(sums / depth + epsilon)[:, None]
    queries = (total[:, :kw] * keys ** (-0.5)).reshape(seqs, heads, keys)
    new_keys = total[:, kw: 2 * kw].reshape(seqs, heads, keys)
    retain = jax.nn.sigmoid(total[:, 2 * kw: 3 * kw] + decay_offset).reshape(seqs, heads, keys)
    values = total[:, 3 * kw: 3 * kw + vw].reshape(seqs, heads, vals)
    gates = total[:, 3 * kw + vw: 3 * kw + 2 * vw]
    new_state = retain[..., None] * state + new_keys[..., None] * values[:, :, None, :]
    read = jnp.einsum("bhk,bhkv->bhv", queries, new_state, precision=lax.Precision.HIGHEST)
    read = read * lax.rsqrt(jnp.mean(read * read, axis=2, keepdims=True) + epsilon) * head_gain
    gated = (read.reshape(seqs, vw) * jax.nn.silu(gates)).astype(bf16)
    gated = lax.all_gather(gated, "kv", axis=0, tiled=True)
    branch = jnp.dot(gated, w_out, preferred_element_type=f32)
    branch = branch + swap_cores(branch.astype(bf16)).astype(f32)
    stream_cols = (tok + branch).astype(bf16)
    stream = lax.all_gather(stream_cols, "kv", axis=1, tiled=True).astype(f32)
    scale = lax.rsqrt(jnp.mean(stream * stream, axis=1, keepdims=True) + epsilon)
    normed = (stream * mlp_gain).astype(bf16)
    hidden = jnp.dot(normed, w_up, preferred_element_type=f32) * scale
    squared = jnp.square(jax.nn.relu(hidden)).astype(bf16)
    down = jnp.dot(squared, w_down, preferred_element_type=f32)
    keep, give = pick(down.reshape(rows, kv_size, 2, half).transpose(2, 1, 0, 3))
    pair = keep + swap_cores(give.astype(bf16)).astype(f32)
    down_own = jnp.sum(exchange(pair.astype(bf16)).astype(f32), axis=0)
    stream_own, _ = pick((stream_cols[:, :half], stream_cols[:, half:]))
    return (stream_own.astype(f32) + down_own).astype(bf16), new_state


def shards(kv_size, tokens, state, mix_gain, w_query, w_key, w_decay, w_value, w_gate, *rest):
    steps = fused_steps if tokens.shape[1] % 128 == 0 and kv_size in (4, 8) else plain_steps
    return steps(kv_size, tokens, state, mix_gain, (w_query, w_key, w_decay, w_value, w_gate), *rest)


def solution(mesh):
    kv_size = mesh.shape["kv"]
    in_specs = (
        P("dp", ("kv", "tp")),
        P(("dp", "kv"), "tp", None, None),
        P("kv"),
        P("kv", "tp"),
        P("kv", "tp"),
        P("kv", "tp"),
        P("kv", "tp"),
        P("kv", "tp"),
        P("tp"),
        P(),
        P("tp", "kv"),
        P(),
        P(None, ("kv", "tp")),
        P(("kv", "tp"), None),
    )
    out_specs = (P("dp", ("kv", "tp")), P(("dp", "kv"), "tp", None, None))

    def body(*args):
        return shards(kv_size, *args)

    return jax.shard_map(body, mesh=mesh, in_specs=in_specs, out_specs=out_specs, check_vma=False)
```
